256 devices in a mesh: ep: 128 (over z, y, x), tp: 2 (over core).
Axes of the slice: x: 4, y: 4, z: 8, core: 2. Of those that a mesh axis runs over, the one named last changes fastest.
Arguments:
- tokens: bfloat16 [6144, 2048], P('ep', 'tp'), may hold values from -12 to 12
- conv_state: bfloat16 [6144, 3, 1024], P('ep', None, 'tp'), may hold values from -6 to 6
- hidden_state: float32 [6144, 1024], P('ep', 'tp'), may hold values from -6 to 6
- mixer_gain: float32 [2048], replicated, may hold values from 0.1 to 1.9
- branch_weight: bfloat16 [2048, 1024], P(None, 'tp'), may hold values from -0.125 to 0.125
- gelu_weight: bfloat16 [2048, 1024], P(None, 'tp'), may hold values from -0.125 to 0.125
- conv_kernel: float32 [4, 1024], P(None, 'tp'), may hold values from -3 to 3
- recur_blocks: bfloat16 [16, 64, 64], P('tp'), may hold values from -0.75 to 0.75
- input_blocks: bfloat16 [16, 64, 64], P('tp'), may hold values from -0.75 to 0.75
- decay_rate: float32 [1024], P('tp'), may hold values from 0.002 to 0.1
- output_weight: bfloat16 [1024, 2048], P(None, 'tp'), may hold values from -0.1875 to 0.1875
- expert_gain: float32 [2048], replicated, may hold values from 0.1 to 1.9
- expert_ids: int32 [6144, 2], P('ep'), may hold values from 0 to 127, as said below
- group_prob: float32 [6144], P('ep'), may hold values from 0.25 to 1
- expert_logit: float32 [6144, 2], P('ep'), may hold values from -4 to 4
- expert_gate: bfloat16 [128, 2048, 512], P('ep', None, 'tp'), may hold values from -0.125 to 0.125
- expert_up: bfloat16 [128, 2048, 512], P('ep', None, 'tp'), may hold values from -0.125 to 0.125
- expert_down: bfloat16 [128, 512, 2048], P('ep', 'tp'), may hold values from -0.25 to 0.25
Outputs:
- layer_out: bfloat16 [6144, 2048], P('ep', 'tp')
- new_hidden: float32 [6144, 1024], P('ep', 'tp')
The draws below stay inside these ranges and needn't reach their ends.
Inputs may be any that keep to these rules, and one draw needn't show every extreme that they name: `expert_ids`: the two experts of a row are different and lie in one group of 32 consecutive experts. Within the rows of one index of ep no expert is named more than 2 times, and one expert is named exactly 2 times by the rows of every index of ep.
All inputs are finite; a program needn't handle non-finite values.
Results may differ from the reference program's by a relative error of at most 0.012.
Values may be sent and summed in bfloat16 or wider, within the bound.
No kernel may reach another device: no remote copies, remote signals or barrier semaphores. Data moves between devices by JAX's collectives and lax.ppermute only.
A program may use at most 64 MiB of HBM per device.

```python
import math
import jax
import jax.numpy as jnp
from jax import lax

D = 2048
LRU = 1024
BLOCK = 64
CONV = 4
FF = 512
GROUPS = 4
TOP = 2
SEQ_DEV = 48
EXPERTS = 128
EXPERTS_GROUP = 32
CAP = 2
TOKENS = 6144
N_EP = 128
N_TP = 2


def draw_tokens(key, part):
    first_key = jax.random.fold_in(key, 0)
    columns = jnp.arange(D, dtype=jnp.float32) / (D - 1)
    column_scale = jnp.exp(jnp.log(0.5) + jnp.log(4.0) * columns)
    values = jnp.clip(jax.random.normal(first_key, (TOKENS, D), jnp.float32), -3.0, 3.0)
    return (values * column_scale[None, :]).astype(jnp.bfloat16)


def draw_expert_ids(key, part):
    devices = TOKENS // SEQ_DEV
    hot_key, round_key, score_key, shuffle_key = jax.random.split(jax.random.fold_in(key, 7), 4)
    hot_expert = jax.random.randint(hot_key, (), 0, EXPERTS)
    round_keys = jax.random.split(round_key, devices * GROUPS * CAP)
    orders = jax.vmap(lambda single: jax.random.permutation(single, EXPERTS_GROUP))(round_keys)
    orders = orders.reshape(devices, GROUPS, CAP, EXPERTS_GROUP).astype(jnp.int32)
    group_base = (jnp.arange(GROUPS, dtype=jnp.int32) * EXPERTS_GROUP)[None, :, None, None]
    members = (orders + group_base).reshape(devices, GROUPS * CAP * (EXPERTS_GROUP // 2), 2)
    candidates = members.shape[1]
    is_hot = jnp.any(members == hot_expert, axis=2).astype(jnp.int32)
    scores = jax.random.randint(score_key, (devices, candidates), 0, 1 << 16)
    keyed = scores * candidates + jnp.arange(candidates, dtype=jnp.int32)[None, :] + (1 - is_hot) * (1 << 29)
    order = jnp.argsort(keyed, axis=1)[:, :SEQ_DEV]
    chosen = jnp.take_along_axis(members, order[:, :, None], axis=1)
    shuffles = jax.vmap(lambda single: jax.random.permutation(single, SEQ_DEV))(jax.random.split(shuffle_key, devices))
    shuffled = jnp.take_along_axis(chosen, shuffles[:, :, None].astype(jnp.int32), axis=1)
    return shuffled.reshape(TOKENS, 2).astype(jnp.int32)


def levels(key, dims, cuts, low, largest):
    def one(axis_at, shards_of):
        heights = jax.random.uniform(jax.random.fold_in(jax.random.fold_in(key, 6), axis_at), (shards_of,), jnp.float32, low / len(cuts), largest / len(cuts))
        return jnp.repeat(jnp.exp(heights), dims[axis_at] // shards_of).reshape((-1,) + (1,) * (len(dims) - axis_at - 1))

    factor_of = one(*cuts[0])
    for cut in cuts[1:]:
        factor_of = factor_of * one(*cut)
    return factor_of


def centred(own_key, extent, scale, limit, pieces=(), kind=jnp.bfloat16):
    loudness = levels(own_key, extent, pieces, -0.22, 0.18) if pieces else 1.0
    entries = jax.random.normal(own_key, extent, jnp.float32) * scale * loudness
    return jnp.minimum(jnp.maximum(entries, -limit), limit).astype(kind)


def setup_inputs(seed: int = 0) -> dict:
    key_list = jax.random.split(jax.random.key(seed), 19)
    return {
        "tokens": draw_tokens(jax.random.fold_in(key_list[18], 71), 0),
        "conv_state": centred(key_list[1], (TOKENS, CONV - 1, LRU), 1.0, 6.0, ((0, 128), (2, 2))),
        "hidden_state": centred(key_list[2], (TOKENS, LRU), 1.0, 6.0, ((0, 128), (1, 2)), jnp.float32),
        "mixer_gain": jnp.clip(1.0 + 0.18 * jax.random.normal(key_list[3], (D,), jnp.float32), 0.1, 1.9),
        "branch_weight": centred(key_list[4], (D, LRU), D ** -0.5, 0.125, ((1, 2),)),
        "gelu_weight": centred(key_list[5], (D, LRU), D ** -0.5, 0.125, ((1, 2),)),
        "conv_kernel": centred(key_list[6], (CONV, LRU), CONV ** -0.5, 3.0, ((1, 2),), jnp.float32),
        "recur_blocks": centred(key_list[7], (LRU // BLOCK, BLOCK, BLOCK), BLOCK ** -0.5, 0.75, ((0, 2),)),
        "input_blocks": centred(key_list[8], (LRU // BLOCK, BLOCK, BLOCK), BLOCK ** -0.5, 0.75, ((0, 2),)),
        "decay_rate": jnp.clip(jnp.exp(math.log(0.1) - 3.912023 * jax.random.uniform(key_list[9], (LRU,), jnp.float32) ** levels(key_list[9], (LRU,), ((0, 2),), -0.2, 0.2)), 0.002, 0.1),
        "output_weight": centred(key_list[10], (LRU, D), LRU ** -0.5, 0.1875, ((1, 2),)),
        "expert_gain": jnp.clip(1.0 + 0.18 * jax.random.normal(key_list[11], (D,), jnp.float32), 0.1, 1.9),
        "expert_ids": draw_expert_ids(jax.random.fold_in(key_list[18], 71), 0),
        "group_prob": jnp.clip(0.25 + 0.75 * jax.random.uniform(key_list[13], (TOKENS,), jnp.float32) ** levels(key_list[13], (TOKENS,), ((0, 128),), -0.2, 0.2), 0.25, 1.0),
        "expert_logit": centred(key_list[14], (TOKENS, TOP), 1.0, 4.0, ((0, 128),), jnp.float32),
        "expert_gate": centred(key_list[15], (EXPERTS, D, FF), D ** -0.5, 0.125, ((0, 128), (2, 2))),
        "expert_up": centred(key_list[16], (EXPERTS, D, FF), D ** -0.5, 0.125, ((0, 128), (2, 2))),
        "expert_down": centred(key_list[17], (EXPERTS, FF, D), FF ** -0.5, 0.25, ((0, 128), (1, 2))),
    }


EPSILON = 1e-06
RATE_SCALE = 8.0

def normalize(values, gain_row):
    squares = lax.optimization_barrier(jnp.mean(values * values, axis=-1, keepdims=True))
    return values * lax.rsqrt(squares + EPSILON) * gain_row

def reference(tokens, conv_state, hidden_state, mixer_gain, branch_weight, gelu_weight, conv_kernel, recur_blocks, input_blocks, decay_rate, output_weight, expert_gain, expert_ids, group_prob, expert_logit, expert_gate, expert_up, expert_down):
    normed = normalize(tokens.astype(jnp.float32), mixer_gain).astype(jnp.bfloat16)
    branch = jnp.dot(normed, branch_weight, preferred_element_type=jnp.float32).astype(jnp.bfloat16)
    gelu_input = jnp.dot(normed, gelu_weight, preferred_element_type=jnp.float32).astype(jnp.bfloat16)
    window = jnp.concatenate([conv_state, branch[:, None, :]], axis=1).astype(jnp.float32)
    convolved = lax.optimization_barrier(jnp.sum(window * conv_kernel[None], axis=1)).astype(jnp.bfloat16)
    grouped = convolved.reshape(TOKENS, LRU // BLOCK, BLOCK).astype(jnp.float32)
    recur_pre = jnp.einsum('tnc,ncd->tnd', grouped, recur_blocks.astype(jnp.float32)).reshape(TOKENS, LRU)
    input_pre = jnp.einsum('tnc,ncd->tnd', grouped, input_blocks.astype(jnp.float32)).reshape(TOKENS, LRU)
    recur_gate = jax.nn.sigmoid(recur_pre)
    input_gate = jax.nn.sigmoid(input_pre)
    log_decay = -RATE_SCALE * recur_gate * decay_rate
    new_hidden = jnp.exp(log_decay) * hidden_state + jnp.sqrt(-jnp.expm1(2.0 * log_decay)) * (input_gate * convolved.astype(jnp.float32))
    mixed_rows = (new_hidden * jax.nn.gelu(gelu_input.astype(jnp.float32), approximate=True)).astype(jnp.bfloat16)
    residual = (tokens.astype(jnp.float32) + jnp.dot(mixed_rows, output_weight, preferred_element_type=jnp.float32)).astype(jnp.bfloat16)
    moe_input = normalize(residual.astype(jnp.float32), expert_gain).astype(jnp.bfloat16)
    sources = jnp.arange(TOKENS * TOP, dtype=jnp.int32) // (SEQ_DEV * TOP)
    block_ids = expert_ids.reshape(N_EP, SEQ_DEV * TOP)
    onehot_ids = (block_ids[:, :, None] == jnp.arange(EXPERTS, dtype=jnp.int32)[None, None, :]).astype(jnp.int32)
    earlier = jnp.cumsum(onehot_ids, axis=1) - onehot_ids
    ranking = lax.optimization_barrier(jnp.sum(earlier * onehot_ids, axis=2)).reshape(-1)
    flat_ids = expert_ids.reshape(-1)
    slot_index = flat_ids * (N_EP * CAP) + sources * CAP + ranking
    token_index = jnp.arange(TOKENS * TOP, dtype=jnp.int32) // TOP
    table = jnp.full((EXPERTS * N_EP * CAP,), TOKENS, jnp.int32).at[slot_index].set(token_index).reshape(EXPERTS, N_EP * CAP)
    padded = jnp.concatenate([moe_input, jnp.zeros((1, D), jnp.bfloat16)], axis=0)

    def one_expert(operands):
        indices, gate_matrix, upper_matrix, down_matrix = operands
        gathered = jnp.take(padded, indices, axis=0)
        gate_part = jnp.dot(gathered, gate_matrix, preferred_element_type=jnp.float32)
        upper_part = jnp.dot(gathered, upper_matrix, preferred_element_type=jnp.float32)
        hidden_units = (jax.nn.silu(gate_part) * upper_part).astype(jnp.bfloat16)
        split_width = FF // N_TP
        total = jnp.zeros((N_EP * CAP, D), jnp.float32)
        for member in range(N_TP):
            piece = jnp.dot(hidden_units[:, member * split_width:(member + 1) * split_width], down_matrix[member * split_width:(member + 1) * split_width], preferred_element_type=jnp.float32)
            total = total + piece.astype(jnp.bfloat16).astype(jnp.float32)
        return total.astype(jnp.bfloat16)
    outcome = lax.map(one_expert, (table, expert_gate, expert_up, expert_down))
    picked = jnp.take(outcome.reshape(EXPERTS * N_EP * CAP, D), slot_index, axis=0).reshape(TOKENS, TOP, D)
    logit_exp = jnp.exp(expert_logit)
    weights = group_prob[:, None] * logit_exp / lax.optimization_barrier(jnp.sum(logit_exp, axis=1, keepdims=True))
    layer_out = (residual.astype(jnp.float32) + lax.optimization_barrier(jnp.sum(weights[:, :, None] * picked.astype(jnp.float32), axis=1))).astype(jnp.bfloat16)
    return (layer_out, new_hidden)
```

```python
import jax
import jax.numpy as jnp
from jax import lax
from jax.sharding import PartitionSpec as P

EPSILON = 1e-06
RATE_SCALE = 8.0


def swap(array):
    return lax.ppermute(array, "tp", [(0, 1), (1, 0)])


def whole_row(own, first):
    other = swap(own)
    return jnp.concatenate(
        [jnp.where(first, own, other), jnp.where(first, other, own)], axis=1
    )


def normalize(values, gain_row):
    squares = jnp.mean(values * values, axis=-1, keepdims=True)
    return values * lax.rsqrt(squares + EPSILON) * gain_row


def local(
    tokens,
    conv_state,
    hidden_state,
    mixer_gain,
    branch_weight,
    gelu_weight,
    conv_kernel,
    recur_blocks,
    input_blocks,
    decay_rate,
    output_weight,
    expert_gain,
    expert_ids,
    group_prob,
    expert_logit,
    expert_gate,
    expert_up,
    expert_down,
):
    first = lax.axis_index("tp") == 0
    experts = lax.axis_size("ep")
    cores = lax.axis_size("tp")
    bf16 = jnp.bfloat16
    whole_tokens = whole_row(tokens, first)
    gates = (expert_gate[0], swap(expert_gate[0]))
    uppers = (expert_up[0], swap(expert_up[0]))
    downs = (expert_down[0], swap(expert_down[0]))

    normed = normalize(whole_tokens.astype(jnp.float32), mixer_gain).astype(bf16)
    branch = jnp.dot(normed, branch_weight, preferred_element_type=jnp.float32).astype(bf16)
    gelu_input = jnp.dot(normed, gelu_weight, preferred_element_type=jnp.float32).astype(bf16)
    taps = conv_kernel.shape[0]
    mixed_taps = branch.astype(jnp.float32) * conv_kernel[taps - 1]
    for tap in range(taps - 1):
        mixed_taps = mixed_taps + conv_state[:, tap].astype(jnp.float32) * conv_kernel[tap]
    convolved = mixed_taps.astype(bf16)
    sequences, channels = convolved.shape
    blocks, block_size = (recur_blocks.shape[0], recur_blocks.shape[1])
    grouped = convolved.reshape(sequences, blocks, block_size)
    recur_pre = jnp.einsum(
        "tnc,ncd->tnd", grouped, recur_blocks, preferred_element_type=jnp.float32
    ).reshape(sequences, channels)
    input_pre = jnp.einsum(
        "tnc,ncd->tnd", grouped, input_blocks, preferred_element_type=jnp.float32
    ).reshape(sequences, channels)
    recur_gate = jax.nn.sigmoid(recur_pre)
    input_gate = jax.nn.sigmoid(input_pre)
    log_decay = -RATE_SCALE * recur_gate * decay_rate
    new_hidden = jnp.exp(log_decay) * hidden_state + jnp.sqrt(-jnp.expm1(2.0 * log_decay)) * (
        input_gate * convolved.astype(jnp.float32)
    )
    mixed_rows = (
        new_hidden * jax.nn.gelu(gelu_input.astype(jnp.float32), approximate=True)
    ).astype(bf16)
    mixed_whole = whole_row(mixed_rows, first)
    residual = (
        tokens.astype(jnp.float32)
        + jnp.dot(mixed_whole, output_weight, preferred_element_type=jnp.float32)
    ).astype(bf16)

    flat_ids = expert_ids.reshape(-1)
    places = jnp.arange(flat_ids.shape[0], dtype=jnp.int32)
    same = (flat_ids[:, None] == flat_ids[None, :]) & (places[None, :] < places[:, None])
    ranking = jnp.sum(same.astype(jnp.int32), axis=1)
    slots = (ranking * experts + flat_ids).reshape(expert_ids.shape)
    slot_list = jnp.arange(cores * experts, dtype=jnp.int32)
    placing = jnp.any(slot_list[:, None, None] == slots[None], axis=2).astype(bf16)
    outgoing = jnp.dot(placing, residual, preferred_element_type=jnp.float32).astype(bf16)
    received = lax.all_to_all(outgoing, ("tp", "ep"), split_axis=0, concat_axis=0, tiled=True)

    half_width = received.shape[1]
    halves = received.reshape(cores, experts, half_width)
    parts = [halves[side].astype(jnp.float32) for side in range(cores)]
    squares = sum(jnp.sum(part * part, axis=1, keepdims=True) for part in parts)
    scaling = lax.rsqrt(squares / (half_width * cores) + EPSILON)
    rows = jnp.concatenate(parts, axis=1) * scaling * expert_gain[None, :]
    rows = rows.astype(bf16)
    results = []
    for gate_matrix, upper_matrix, down_matrix in zip(gates, uppers, downs):
        gate_part = jnp.dot(rows, gate_matrix, preferred_element_type=jnp.float32)
        upper_part = jnp.dot(rows, upper_matrix, preferred_element_type=jnp.float32)
        hidden_units = (jax.nn.silu(gate_part) * upper_part).astype(bf16)
        results.append((hidden_units, down_matrix))
    answers = []
    for side in range(cores):
        span = slice(side * half_width, (side + 1) * half_width)
        total = sum(
            jnp.dot(hidden_units, down_matrix[:, span], preferred_element_type=jnp.float32)
            for hidden_units, down_matrix in results
        )
        answers.append(total.astype(bf16))
    answers = jnp.concatenate(answers, axis=0)
    returned = lax.all_to_all(answers, ("tp", "ep"), split_axis=0, concat_axis=0, tiled=True)

    logit_exp = jnp.exp(expert_logit)
    weights = group_prob[:, None] * logit_exp / jnp.sum(logit_exp, axis=1, keepdims=True)
    picking = jnp.sum(
        jnp.where(slots[:, :, None] == slot_list[None, None, :], weights[:, :, None], 0.0), axis=1
    )
    high = picking.astype(bf16)
    low = (picking - high.astype(jnp.float32)).astype(bf16)
    chosen = jnp.dot(high, returned, preferred_element_type=jnp.float32) + jnp.dot(
        low, returned, preferred_element_type=jnp.float32
    )
    layer_out = (residual.astype(jnp.float32) + chosen).astype(bf16)
    return (layer_out, new_hidden)


def solution(mesh):
    return jax.shard_map(
        local,
        mesh=mesh,
        in_specs=(
            P("ep", "tp"),
            P("ep", None, "tp"),
            P("ep", "tp"),
            P(),
            P(None, "tp"),
            P(None, "tp"),
            P(None, "tp"),
            P("tp", None, None),
            P("tp", None, None),
            P("tp"),
            P(None, "tp"),
            P(),
            P("ep", None),
            P("ep"),
            P("ep", None),
            P("ep", None, "tp"),
            P("ep", None, "tp"),
            P("ep", "tp", None),
        ),
        out_specs=(P("ep", "tp"), P("ep", "tp")),
        check_vma=False,
    )
```

```python
import jax
import jax.numpy as jnp
from jax import lax
from jax.experimental import pallas as pl
from jax.experimental.pallas import tpu as pltpu
from jax.sharding import PartitionSpec as P

EPSILON = 1e-06
RATE_SCALE = 8.0
BF16 = jnp.bfloat16
F32 = jnp.float32


def swap(array):
    return lax.ppermute(array, "tp", [(0, 1), (1, 0)])


def iota(shape, dim):
    return lax.broadcasted_iota(jnp.int32, shape, dim)


def mm(left, right):
    return jnp.dot(left, right, preferred_element_type=F32)


def call(body, outs, smem=0):
    def run(*operands):
        specs = [
            pl.BlockSpec(memory_space=pltpu.SMEM if at < smem else pltpu.VMEM)
            for at in range(len(operands))
        ]
        return pl.pallas_call(
            body,
            out_shape=tuple(jax.ShapeDtypeStruct(shape, kind) for shape, kind in outs),
            in_specs=specs,
            out_specs=tuple(pl.BlockSpec(memory_space=pltpu.VMEM) for _ in outs),
            scratch_shapes=getattr(body, "scratch", ()),
            name=body.__name__,
            compiler_params=pltpu.CompilerParams(vmem_limit_bytes=body.room << 20),
        )(*operands)

    return run


def block_diagonal(blocks):
    count, size, _ = blocks.shape
    width = count * size
    tiled = (iota((size, width), 1) % size == iota((size, width), 0)).astype(BF16)
    spread = mm(blocks.reshape(width, size), tiled)
    keep = iota((width, width), 0) // size == iota((width, width), 1) // size
    return jnp.where(keep, spread, 0.0).astype(BF16)


def prepare(recur_ref, input_ref, ids_ref, prob_ref, logit_ref, rd_ref, id_ref, place_ref, pick_ref):
    rd_ref[...] = block_diagonal(recur_ref[...])
    id_ref[...] = block_diagonal(input_ref[...])
    ids = ids_ref[...]
    sequences, top_count = ids.shape
    experts = 128
    lane = iota((sequences, experts), 1)
    onehots = [(ids[:, k : k + 1] == lane).astype(F32) for k in range(top_count)]
    before = (iota((sequences, sequences), 1) < iota((sequences, sequences), 0)).astype(BF16)
    earlier = mm(before, sum(onehots).astype(BF16))
    ranks = [jnp.sum(earlier * one, axis=1, keepdims=True).astype(jnp.int32) for one in onehots]
    logit_exp = jnp.exp(logit_ref[...])
    diagonal = iota((sequences, sequences), 0) == iota((sequences, sequences), 1)
    prob = jnp.sum(jnp.where(diagonal, prob_ref[...], 0.0), axis=1, keepdims=True)
    weights = prob * logit_exp / jnp.sum(logit_exp, axis=1, keepdims=True)
    columns = 4 * experts
    column = iota((sequences, columns), 1)
    for half in range(2):
        place = jnp.zeros((sequences, columns), F32)
        pick = jnp.zeros((sequences, columns), F32)
        for k in range(top_count):
            row = (ranks[k] * experts + ids[:, k : k + 1]) * 2 + half
            here = column == row
            place = jnp.where(here, 1.0, place)
            pick = jnp.where(here, weights[:, k : k + 1], pick)
        span = slice(half * sequences, (half + 1) * sequences)
        place_ref[span, :] = place.astype(BF16)
        high = pick.astype(BF16)
        pick_ref[span, :] = high
        low_span = slice((2 + half) * sequences, (3 + half) * sequences)
        pick_ref[low_span, :] = (pick - high.astype(F32)).astype(BF16)


def expm1(values):
    series = values * (
        1.0
        + values
        * (1 / 2 + values * (1 / 6 + values * (1 / 24 + values * (1 / 120 + values * (1 / 720)))))
    )
    return jnp.where(jnp.abs(values) < 0.25, series, jnp.exp(values) - 1.0)


def mixer(
    core_ref, own_ref, other_ref, gain_ref, branch_ref, gelu_ref, state_ref, taps_ref,
    hidden_ref, rd_ref, id_ref, rate_ref, new_ref, mixed_ref,
):
    core = core_ref[0]
    own = own_ref[...].astype(F32)
    other = other_ref[...].astype(F32)
    half = own.shape[1]
    squares = jnp.sum(own * own + other * other, axis=1, keepdims=True)
    scaling = lax.rsqrt(squares / (2 * half) + EPSILON)
    left, right = gain_ref[:, :half], gain_ref[:, half:]
    own = (own * scaling * jnp.where(core == 0, left, right)).astype(BF16)
    other = (other * scaling * jnp.where(core == 0, right, left)).astype(BF16)
    own_rows = pl.ds(pl.multiple_of(core * half, half), half)
    other_rows = pl.ds(pl.multiple_of((1 - core) * half, half), half)
    branch = (mm(own, branch_ref[own_rows, :]) + mm(other, branch_ref[other_rows, :])).astype(BF16)
    gelu_input = (mm(own, gelu_ref[own_rows, :]) + mm(other, gelu_ref[other_rows, :])).astype(BF16)
    taps = taps_ref.shape[0]
    convolved = branch.astype(F32) * taps_ref[taps - 1 : taps, :]
    for tap in range(taps - 1):
        convolved = convolved + state_ref[:, tap, :].astype(F32) * taps_ref[tap : tap + 1, :]
    convolved = convolved.astype(BF16)
    recur_gate = jax.nn.sigmoid(mm(convolved, rd_ref[...]))
    input_gate = jax.nn.sigmoid(mm(convolved, id_ref[...]))
    log_decay = -RATE_SCALE * recur_gate * rate_ref[...]
    new_hidden = jnp.exp(log_decay) * hidden_ref[...] + jnp.sqrt(-expm1(2.0 * log_decay)) * (
        input_gate * convolved.astype(F32)
    )
    new_ref[...] = new_hidden
    mixed_ref[...] = (new_hidden * jax.nn.gelu(gelu_input.astype(F32), approximate=True)).astype(BF16)


def project(core_ref, tokens_ref, own_ref, other_ref, weight_ref, place_ref, residual_ref, out_ref):
    core = core_ref[0]
    half = own_ref.shape[1]
    own_rows = pl.ds(pl.multiple_of(core * half, half), half)
    other_rows = pl.ds(pl.multiple_of((1 - core) * half, half), half)
    product = mm(own_ref[...], weight_ref[own_rows, :]) + mm(other_ref[...], weight_ref[other_rows, :])
    residual = (tokens_ref[...].astype(F32) + product).astype(BF16)
    residual_ref[...] = residual
    width = residual.shape[1] // 2
    stacked = jnp.concatenate([residual[:, :width], residual[:, width:]], axis=0)
    out_ref[...] = lax.dot_general(
        place_ref[...], stacked, (((0,), (0,)), ((), ())), preferred_element_type=F32
    ).astype(BF16)


def experts_of(
    rows_ref, gain_ref, gate_a, gate_b, up_a, up_b, down_a, down_b, out_ref, scratch_ref
):
    total, width = rows_ref.shape
    slots = total // 4
    pieces = width // 128
    for piece in range(pieces):
        scratch_ref[piece] = rows_ref[:, piece * 128 : (piece + 1) * 128].astype(F32)

    def of_quarter(q):
        return pl.ds((q // 2) * 2 * slots + q % 2, slots, 2)

    quarters = [
        jnp.concatenate([scratch_ref[piece, of_quarter(q), :] for piece in range(pieces)], axis=1)
        for q in range(4)
    ]
    squares = sum(jnp.sum(part * part, axis=1, keepdims=True) for part in quarters)
    scaling = lax.rsqrt(squares / (4 * width) + EPSILON)
    quarters = [
        (part * scaling * gain_ref[:, q * width : (q + 1) * width]).astype(BF16)
        for q, part in enumerate(quarters)
    ]
    rows = jnp.concatenate(quarters, axis=1)
    hidden = []
    for gate_ref, up_ref in ((gate_a, up_a), (gate_b, up_b)):
        gate = mm(rows, gate_ref[...])
        up = mm(rows, up_ref[...])
        hidden.append((jax.nn.silu(gate) * up).astype(BF16))
    for q in range(4):
        span = slice(q * width, (q + 1) * width)
        answer = mm(hidden[0], down_a[:, span]) + mm(hidden[1], down_b[:, span])
        for piece in range(pieces):
            scratch_ref[piece, of_quarter(q), :] = answer[:, piece * 128 : (piece + 1) * 128]
    for piece in range(pieces):
        out_ref[:, piece * 128 : (piece + 1) * 128] = scratch_ref[piece].astype(BF16)


experts_of.scratch = (pltpu.VMEM((4, 512, 128), F32),)


def combine(returned_ref, pick_ref, residual_ref, out_ref):
    found = mm(pick_ref[...], returned_ref[...])
    sequences, width = residual_ref.shape
    width = width // 2
    for half in range(2):
        span = slice(half * width, (half + 1) * width)
        high = found[half * sequences : (half + 1) * sequences]
        low = found[(2 + half) * sequences : (3 + half) * sequences]
        out_ref[:, span] = (residual_ref[:, span].astype(F32) + (high + low)).astype(BF16)


prepare.room, mixer.room, project.room, experts_of.room, combine.room = 8, 16, 8, 20, 8


def exchange(rows):
    total, width = rows.shape
    messages = rows.reshape(total // 2, 2, width)
    arrived = lax.all_to_all(messages, ("tp", "ep"), split_axis=0, concat_axis=0, tiled=True)
    return arrived.reshape(total, width)


def local(
    tokens,
    conv_state,
    hidden_state,
    mixer_gain,
    branch_weight,
    gelu_weight,
    conv_kernel,
    recur_blocks,
    input_blocks,
    decay_rate,
    output_weight,
    expert_gain,
    expert_ids,
    group_prob,
    expert_logit,
    expert_gate,
    expert_up,
    expert_down,
):
    core = lax.axis_index("tp").astype(jnp.int32).reshape(1)
    sequences, half = tokens.shape
    channels = hidden_state.shape[1]
    messages = 2 * lax.axis_size("ep") * lax.axis_size("tp")
    width = half // 2

    other_tokens = swap(tokens)
    recur_full, input_full, place, pick = call(
        prepare,
        (
            ((channels, channels), BF16),
            ((channels, channels), BF16),
            ((2 * sequences, messages), BF16),
            ((4 * sequences, messages), BF16),
        ),
    )(recur_blocks, input_blocks, expert_ids, group_prob[None, :], expert_logit)
    new_hidden, mixed = call(
        mixer, (((sequences, channels), F32), ((sequences, channels), BF16)), smem=1
    )(
        core, tokens, other_tokens, mixer_gain[None, :], branch_weight, gelu_weight,
        conv_state, conv_kernel, hidden_state, recur_full, input_full, decay_rate[None, :],
    )
    other_mixed = swap(mixed)
    residual, outgoing = call(
        project, (((sequences, half), BF16), ((messages, width), BF16)), smem=1
    )(core, tokens, mixed, other_mixed, output_weight, place)
    other_gate, other_up, other_down = swap(expert_gate[0]), swap(expert_up[0]), swap(expert_down[0])
    received = exchange(outgoing)
    (answers,) = call(experts_of, (((messages, width), BF16),))(
        received, expert_gain[None, :], expert_gate[0], other_gate, expert_up[0], other_up,
        expert_down[0], other_down,
    )
    returned = exchange(answers)
    (layer_out,) = call(combine, (((sequences, half), BF16),))(returned, pick, residual)
    return (layer_out, new_hidden)


def solution(mesh):
    return jax.shard_map(
        local,
        mesh=mesh,
        in_specs=(
            P("ep", "tp"),
            P("ep", None, "tp"),
            P("ep", "tp"),
            P(),
            P(None, "tp"),
            P(None, "tp"),
            P(None, "tp"),
            P("tp", None, None),
            P("tp", None, None),
            P("tp"),
            P(None, "tp"),
            P(),
            P("ep", None),
            P("ep"),
            P("ep", None),
            P("ep", None, "tp"),
            P("ep", None, "tp"),
            P("ep", "tp", None),
        ),
        out_specs=(P("ep", "tp"), P("ep", "tp")),
        check_vma=False,
    )
```

```python
import jax
import jax.numpy as jnp
from jax import lax
from jax.experimental import pallas as pl
from jax.experimental.pallas import tpu as pltpu
from jax.sharding import PartitionSpec as P

EPSILON = 1e-06
RATE_SCALE = 8.0
BF16 = jnp.bfloat16
F32 = jnp.float32


def swap(array):
    return lax.ppermute(array, "tp", [(0, 1), (1, 0)])


def iota(shape, dim):
    return lax.broadcasted_iota(jnp.int32, shape, dim)


def mm(left, right):
    return jnp.dot(left, right, preferred_element_type=F32)


def call(body, outs, spaces):
    places = {"s": pltpu.SMEM, "v": pltpu.VMEM, "V": pltpu.VMEM, "h": pltpu.HBM}
    run = pl.pallas_call(
        body,
        out_shape=tuple(jax.ShapeDtypeStruct(shape, kind) for shape, kind in outs),
        in_specs=[pl.BlockSpec(memory_space=places[space]) for space in spaces],
        out_specs=tuple(pl.BlockSpec(memory_space=pltpu.VMEM) for _ in outs),
        scratch_shapes=getattr(body, "scratch", ()),
        name=body.__name__,
        compiler_params=pltpu.CompilerParams(vmem_limit_bytes=body.room << 20),
    )

    def placed(*operands):
        return run(
            *(
                pltpu.with_memory_space_constraint(operand, places[space])
                if space in "Vh"
                else operand
                for operand, space in zip(operands, spaces)
            )
        )

    return placed


def half_of(ref, core, other, dim):
    size = ref.shape[dim] // 2
    start = (1 - core if other else core) * size
    span = pl.ds(pl.multiple_of(start, size), size)
    return ref.at[span, :] if dim == 0 else ref.at[:, span]


def block_diagonal(blocks):
    count, size, _ = blocks.shape
    width = count * size
    tiled = (iota((size, width), 1) % size == iota((size, width), 0)).astype(BF16)
    spread = mm(blocks.reshape(width, size), tiled)
    keep = iota((width, width), 0) // size == iota((width, width), 1) // size
    return jnp.where(keep, spread, 0.0).astype(BF16)


def as_column(row):
    size = row.shape[1]
    diagonal = iota((size, size), 0) == iota((size, size), 1)
    return jnp.sum(jnp.where(diagonal, row, 0.0), axis=1, keepdims=True)


def route(ids_ref, prob_ref, logit_ref, place_ref, pick_ref):
    top_count, sequences = ids_ref.shape
    columns = place_ref.shape[1]
    experts = columns // 4
    rows = [ids_ref[k : k + 1, :].astype(F32) for k in range(top_count)]
    ids = [as_column(row).astype(jnp.int32) for row in rows]
    lane = iota((sequences, experts), 1)
    onehots = [(one == lane).astype(F32) for one in ids]
    before = (iota((sequences, sequences), 1) < iota((sequences, sequences), 0)).astype(BF16)
    earlier = mm(before, sum(onehots).astype(BF16))
    ranks = [jnp.sum(earlier * one, axis=1, keepdims=True).astype(jnp.int32) for one in onehots]
    logit_exp = [jnp.exp(logit_ref[k : k + 1, :]) for k in range(top_count)]
    weights = [as_column(prob_ref[...] * one / sum(logit_exp)) for one in logit_exp]
    column = iota((sequences, columns), 1)
    for half in range(2):
        place = jnp.zeros((sequences, columns), F32)
        pick = jnp.zeros((sequences, columns), F32)
        for k in range(top_count):
            here = column == (ranks[k] * experts + ids[k]) * 2 + half
            place = jnp.where(here, 1.0, place)
            pick = jnp.where(here, weights[k], pick)
        span = slice(half * sequences, (half + 1) * sequences)
        place_ref[span, :] = place.astype(BF16)
        high = pick.astype(BF16)
        pick_ref[span, :] = high
        low_span = slice((2 + half) * sequences, (3 + half) * sequences)
        pick_ref[low_span, :] = (pick - high.astype(F32)).astype(BF16)


def begin(
    core_ref, tokens_hbm, gain_hbm, branch_hbm, gelu_hbm, recur_hbm, input_hbm, ids_hbm, prob_hbm,
    logit_hbm, state_hbm, taps_hbm, hidden_hbm, rate_hbm,
    tokens_ref, gain_ref, branch_ref, gelu_ref, state_ref, taps_ref, hidden_ref, rate_ref,
    rd_ref, id_ref, place_ref, pick_ref, branch_part, gelu_part, squares_ref,
    own_gain, own_branch, own_gelu, recur_ref, input_ref, ids_ref, prob_ref, logit_ref, sems,
):
    core = core_ref[0]
    pairs = (
        (tokens_hbm, tokens_ref),
        (half_of(gain_hbm, core, False, 1), own_gain),
        (half_of(branch_hbm, core, False, 0), own_branch),
        (half_of(gelu_hbm, core, False, 0), own_gelu),
        (ids_hbm, ids_ref),
        (prob_hbm, prob_ref),
        (logit_hbm, logit_ref),
        (recur_hbm, recur_ref),
        (input_hbm, input_ref),
        (half_of(branch_hbm, core, True, 0), branch_ref),
        (half_of(gelu_hbm, core, True, 0), gelu_ref),
        (half_of(gain_hbm, core, True, 1), gain_ref),
        (state_hbm, state_ref),
        (taps_hbm, taps_ref),
        (hidden_hbm, hidden_ref),
        (rate_hbm, rate_ref),
    )
    copies = [
        pltpu.make_async_copy(source, target, sems.at[at]) for at, (source, target) in enumerate(pairs)
    ]
    for copy in copies:
        copy.start()
    for copy in copies[4:7]:
        copy.wait()
    route(ids_ref, prob_ref, logit_ref, place_ref, pick_ref)
    for copy in copies[7:9]:
        copy.wait()
    rd_ref[...] = block_diagonal(recur_ref[...])
    id_ref[...] = block_diagonal(input_ref[...])
    for copy in copies[:2]:
        copy.wait()
    own = tokens_ref[...].astype(F32)
    squares_ref[...] = jnp.sum(own * own, axis=1, keepdims=True)
    own = (own * own_gain[...]).astype(BF16)
    copies[2].wait()
    branch_part[...] = mm(own, own_branch[...])
    copies[3].wait()
    gelu_part[...] = mm(own, own_gelu[...])
    for copy in copies[9:]:
        copy.wait()


begin.scratch = (
    pltpu.VMEM((1, 1024), F32),
    pltpu.VMEM((1024, 512), BF16),
    pltpu.VMEM((1024, 512), BF16),
    pltpu.VMEM((8, 64, 64), BF16),
    pltpu.VMEM((8, 64, 64), BF16),
    pltpu.VMEM((2, 48), jnp.int32),
    pltpu.VMEM((1, 48), F32),
    pltpu.VMEM((2, 48), F32),
    pltpu.SemaphoreType.DMA((16,)),
)


def expm1(values):
    series = values * (
        1.0
        + values
        * (1 / 2 + values * (1 / 6 + values * (1 / 24 + values * (1 / 120 + values * (1 / 720)))))
    )
    return jnp.where(jnp.abs(values) < 0.25, series, jnp.exp(values) - 1.0)


def mixer(
    other_ref, squares_ref, gain_ref, branch_ref, gelu_ref, branch_part, gelu_part, state_ref,
    taps_ref, hidden_ref, rate_ref, rd_ref, id_ref, new_ref, mixed_ref,
):
    other = other_ref[...].astype(F32)
    half = other.shape[1]
    squares = squares_ref[...] + jnp.sum(other * other, axis=1, keepdims=True)
    scaling = lax.rsqrt(squares / (2 * half) + EPSILON)
    other = (other * gain_ref[...]).astype(BF16)
    branch = ((branch_part[...] + mm(other, branch_ref[...])) * scaling).astype(BF16)
    gelu_input = ((gelu_part[...] + mm(other, gelu_ref[...])) * scaling).astype(BF16)
    taps = taps_ref.shape[0]
    convolved = branch.astype(F32) * taps_ref[taps - 1 : taps, :]
    for tap in range(taps - 1):
        convolved = convolved + state_ref[tap].astype(F32) * taps_ref[tap : tap + 1, :]
    convolved = convolved.astype(BF16)
    recur_gate = jax.nn.sigmoid(mm(convolved, rd_ref[...]))
    input_gate = jax.nn.sigmoid(mm(convolved, id_ref[...]))
    log_decay = -RATE_SCALE * recur_gate * rate_ref[...]
    new_hidden = jnp.exp(log_decay) * hidden_ref[...] + jnp.sqrt(-expm1(2.0 * log_decay)) * (
        input_gate * convolved.astype(F32)
    )
    new_ref[...] = new_hidden
    mixed_ref[...] = (new_hidden * jax.nn.gelu(gelu_input.astype(F32), approximate=True)).astype(BF16)


def project(core_ref, tokens_ref, own_ref, other_ref, weight_ref, place_ref, residual_ref, out_ref):
    core = core_ref[0]
    half = own_ref.shape[1]
    own_rows = pl.ds(pl.multiple_of(core * half, half), half)
    other_rows = pl.ds(pl.multiple_of((1 - core) * half, half), half)
    product = mm(own_ref[...], weight_ref[own_rows, :]) + mm(other_ref[...], weight_ref[other_rows, :])
    residual = (tokens_ref[...].astype(F32) + product).astype(BF16)
    residual_ref[...] = residual
    width = residual.shape[1] // 2
    stacked = jnp.concatenate([residual[:, :width], residual[:, width:]], axis=0)
    out_ref[...] = lax.dot_general(
        place_ref[...], stacked, (((0,), (0,)), ((), ())), preferred_element_type=F32
    ).astype(BF16)


def experts_of(
    rows_ref, gain_ref, gate_a, up_a, down_a_hbm, gate_b_hbm, up_b_hbm, down_b_hbm, out_ref,
    down_a, gate_b, up_b, down_b, scratch_ref, sems,
):
    pairs = ((gate_b_hbm, gate_b), (up_b_hbm, up_b), (down_a_hbm, down_a), (down_b_hbm, down_b))
    copies = [
        pltpu.make_async_copy(source, target, sems.at[at]) for at, (source, target) in enumerate(pairs)
    ]
    for copy in copies:
        copy.start()
    total, width = rows_ref.shape
    slots = total // 4
    pieces = width // 128
    for piece in range(pieces):
        scratch_ref[piece] = rows_ref[:, piece * 128 : (piece + 1) * 128].astype(F32)

    def of_quarter(q):
        return pl.ds((q // 2) * 2 * slots + q % 2, slots, 2)

    quarters = [
        jnp.concatenate([scratch_ref[piece, of_quarter(q), :] for piece in range(pieces)], axis=1)
        for q in range(4)
    ]
    squares = sum(jnp.sum(part * part, axis=1, keepdims=True) for part in quarters)
    scaling = lax.rsqrt(squares / (4 * width) + EPSILON)
    quarters = [
        (part * scaling * gain_ref[:, q * width : (q + 1) * width]).astype(BF16)
        for q, part in enumerate(quarters)
    ]
    rows = jnp.concatenate(quarters, axis=1)
    hidden = [(jax.nn.silu(mm(rows, gate_a[...])) * mm(rows, up_a[...])).astype(BF16)]
    copies[0].wait()
    gate = jax.nn.silu(mm(rows, gate_b[...]))
    copies[1].wait()
    hidden.append((gate * mm(rows, up_b[...])).astype(BF16))
    copies[2].wait()
    copies[3].wait()
    for q in range(4):
        span = slice(q * width, (q + 1) * width)
        answer = mm(hidden[0], down_a[:, span]) + mm(hidden[1], down_b[:, span])
        for piece in range(pieces):
            scratch_ref[piece, of_quarter(q), :] = answer[:, piece * 128 : (piece + 1) * 128]
    for piece in range(pieces):
        out_ref[:, piece * 128 : (piece + 1) * 128] = scratch_ref[piece].astype(BF16)


experts_of.scratch = (
    pltpu.VMEM((256, 2048), BF16),
    pltpu.VMEM((2048, 256), BF16),
    pltpu.VMEM((2048, 256), BF16),
    pltpu.VMEM((256, 2048), BF16),
    pltpu.VMEM((4, 512, 128), F32),
    pltpu.SemaphoreType.DMA((4,)),
)


def combine(returned_ref, pick_ref, residual_ref, out_ref):
    found = mm(pick_ref[...], returned_ref[...])
    sequences, width = residual_ref.shape
    width = width // 2
    for half in range(2):
        span = slice(half * width, (half + 1) * width)
        high = found[half * sequences : (half + 1) * sequences]
        low = found[(2 + half) * sequences : (3 + half) * sequences]
        out_ref[:, span] = (residual_ref[:, span].astype(F32) + (high + low)).astype(BF16)


begin.room, mixer.room, project.room, experts_of.room, combine.room = 8, 6, 6, 12, 6


def exchange(rows):
    total, width = rows.shape
    messages = rows.reshape(total // 2, 2, width)
    arrived = lax.all_to_all(messages, ("tp", "ep"), split_axis=0, concat_axis=0, tiled=True)
    return arrived.reshape(total, width)


def local(
    tokens,
    conv_state,
    hidden_state,
    mixer_gain,
    branch_weight,
    gelu_weight,
    conv_kernel,
    recur_blocks,
    input_blocks,
    decay_rate,
    output_weight,
    expert_gain,
    expert_ids,
    group_prob,
    expert_logit,
    expert_gate,
    expert_up,
    expert_down,
):
    core = lax.axis_index("tp").astype(jnp.int32).reshape(1)
    sequences, half = tokens.shape
    channels = hidden_state.shape[1]
    messages = 2 * lax.axis_size("ep") * lax.axis_size("tp")
    width = half // 2

    other_tokens = swap(tokens)
    kinds = (
        ((sequences, half), BF16),
        ((1, half), F32),
        ((half, channels), BF16),
        ((half, channels), BF16),
        ((3, sequences, channels), BF16),
        ((4, channels), F32),
        ((sequences, channels), F32),
        ((1, channels), F32),
        ((channels, channels), BF16),
        ((channels, channels), BF16),
        ((2 * sequences, messages), BF16),
        ((4 * sequences, messages), BF16),
        ((sequences, channels), F32),
        ((sequences, channels), F32),
        ((sequences, 1), F32),
    )
    (
        own_tokens, gain, branch_rows, gelu_rows, state, taps, hidden, rate, recur_full, input_full,
        place, pick, branch_part, gelu_part, squares,
    ) = call(begin, kinds, "s" + "h" * 13)(
        core, tokens, mixer_gain[None, :], branch_weight, gelu_weight, recur_blocks, input_blocks,
        expert_ids.T, group_prob[None, :], expert_logit.T, jnp.transpose(conv_state, (1, 0, 2)),
        conv_kernel, hidden_state, decay_rate[None, :],
    )
    new_hidden, mixed = call(
        mixer, (((sequences, channels), F32), ((sequences, channels), BF16)), "v" * 13
    )(
        other_tokens, squares, gain, branch_rows, gelu_rows, branch_part, gelu_part, state, taps,
        hidden, rate, recur_full, input_full,
    )
    other_mixed = swap(mixed)
    residual, outgoing = call(
        project, (((sequences, half), BF16), ((messages, width), BF16)), "s" + "v" * 5
    )(core, own_tokens, mixed, other_mixed, output_weight, place)
    other_gate, other_up, other_down = swap(expert_gate[0]), swap(expert_up[0]), swap(expert_down[0])
    received = exchange(outgoing)
    (answers,) = call(experts_of, (((messages, width), BF16),), "vvvvhhhh")(
        received, expert_gain[None, :], expert_gate[0], expert_up[0], expert_down[0], other_gate,
        other_up, other_down,
    )
    returned = exchange(answers)
    (layer_out,) = call(combine, (((sequences, half), BF16),), "vvv")(returned, pick, residual)
    return (layer_out, new_hidden)


def solution(mesh):
    return jax.shard_map(
        local,
        mesh=mesh,
        in_specs=(
            P("ep", "tp"),
            P("ep", None, "tp"),
            P("ep", "tp"),
            P(),
            P(None, "tp"),
            P(None, "tp"),
            P(None, "tp"),
            P("tp", None, None),
            P("tp", None, None),
            P("tp"),
            P(None, "tp"),
            P(),
            P("ep", None),
            P("ep"),
            P("ep", None),
            P("ep", None, "tp"),
            P("ep", None, "tp"),
            P("ep", "tp", None),
        ),
        out_specs=(P("ep", "tp"), P("ep", "tp")),
        check_vma=False,
    )
```

```python
import jax
import jax.numpy as jnp
from jax import lax
from jax.experimental import pallas as pl
from jax.experimental.pallas import tpu as pltpu
from jax.sharding import PartitionSpec as P

EPSILON = 1e-06
RATE_SCALE = 8.0
BF16 = jnp.bfloat16
F32 = jnp.float32


def swap(array):
    return lax.ppermute(array, "tp", [(0, 1), (1, 0)])


def iota(shape, dim):
    return lax.broadcasted_iota(jnp.int32, shape, dim)


def mm(left, right):
    return jnp.dot(left, right, preferred_element_type=F32)


def call(body, outs, spaces):
    places = {"s": pltpu.SMEM, "v": pltpu.VMEM, "V": pltpu.VMEM, "h": pltpu.HBM}
    run = pl.pallas_call(
        body,
        out_shape=tuple(jax.ShapeDtypeStruct(shape, kind) for shape, kind in outs),
        in_specs=[pl.BlockSpec(memory_space=places[space]) for space in spaces],
        out_specs=tuple(pl.BlockSpec(memory_space=pltpu.VMEM) for _ in outs),
        scratch_shapes=getattr(body, "scratch", ()),
        compiler_params=pltpu.CompilerParams(vmem_limit_bytes=body.room << 20),
    )

    def placed(*operands):
        return run(
            *(
                pltpu.with_memory_space_constraint(operand, places[space])
                if space in "Vh"
                else operand
                for operand, space in zip(operands, spaces)
            )
        )

    return placed


def half_of(ref, core, other, dim):
    size = ref.shape[dim] // 2
    start = (1 - core if other else core) * size
    span = pl.ds(pl.multiple_of(start, size), size)
    return ref.at[span, :] if dim == 0 else ref.at[:, span]


def block_diagonal(blocks):
    count, size, _ = blocks.shape
    width = count * size
    tiled = (iota((size, width), 1) % size == iota((size, width), 0)).astype(BF16)
    spread = mm(blocks.reshape(width, size), tiled)
    keep = iota((width, width), 0) // size == iota((width, width), 1) // size
    return jnp.where(keep, spread, 0.0).astype(BF16)


def as_column(row):
    size = row.shape[1]
    diagonal = iota((size, size), 0) == iota((size, size), 1)
    return jnp.sum(jnp.where(diagonal, row, 0.0), axis=1, keepdims=True)


def route(ids_ref, prob_ref, logit_ref, place_ref, pick_ref):
    top_count, sequences = ids_ref.shape
    columns = place_ref.shape[1]
    experts = columns // 4
    rows = [ids_ref[k : k + 1, :].astype(F32) for k in range(top_count)]
    ids = [as_column(row).astype(jnp.int32) for row in rows]
    lane = iota((sequences, experts), 1)
    onehots = [(one == lane).astype(F32) for one in ids]
    before = (iota((sequences, sequences), 1) < iota((sequences, sequences), 0)).astype(BF16)
    earlier = mm(before, sum(onehots).astype(BF16))
    ranks = [jnp.sum(earlier * one, axis=1, keepdims=True).astype(jnp.int32) for one in onehots]
    logit_exp = [jnp.exp(logit_ref[k : k + 1, :]) for k in range(top_count)]
    weights = [as_column(prob_ref[...] * one / sum(logit_exp)) for one in logit_exp]
    column = iota((sequences, columns), 1)
    for half in range(2):
        place = jnp.zeros((sequences, columns), F32)
        pick = jnp.zeros((sequences, columns), F32)
        for k in range(top_count):
            here = column == (ranks[k] * experts + ids[k]) * 2 + half
            place = jnp.where(here, 1.0, place)
            pick = jnp.where(here, weights[k], pick)
        span = slice(half * sequences, (half + 1) * sequences)
        place_ref[span, :] = place.astype(BF16)
        high = pick.astype(BF16)
        pick_ref[span, :] = high
        low_span = slice((2 + half) * sequences, (3 + half) * sequences)
        pick_ref[low_span, :] = (pick - high.astype(F32)).astype(BF16)


def begin(
    core_ref, tokens_hbm, gain_hbm, branch_hbm, gelu_hbm, recur_hbm, input_hbm, ids_hbm, prob_hbm,
    logit_hbm, state_hbm, taps_hbm, hidden_hbm, rate_hbm,
    tokens_ref, gain_ref, branch_ref, gelu_ref, state_ref, taps_ref, hidden_ref, rate_ref,
    rd_ref, id_ref, place_ref, pick_ref, branch_part, gelu_part, squares_ref,
    own_gain, own_branch, own_gelu, recur_ref, input_ref, ids_ref, prob_ref, logit_ref, sems,
):
    core = core_ref[0]
    pairs = (
        (tokens_hbm, tokens_ref),
        (half_of(gain_hbm, core, False, 1), own_gain),
        (half_of(branch_hbm, core, False, 0), own_branch),
        (half_of(gelu_hbm, core, False, 0), own_gelu),
        (ids_hbm, ids_ref),
        (prob_hbm, prob_ref),
        (logit_hbm, logit_ref),
        (recur_hbm, recur_ref),
        (input_hbm, input_ref),
        (half_of(branch_hbm, core, True, 0), branch_ref),
        (half_of(gelu_hbm, core, True, 0), gelu_ref),
        (half_of(gain_hbm, core, True, 1), gain_ref),
        (state_hbm, state_ref),
        (taps_hbm, taps_ref),
        (hidden_hbm, hidden_ref),
        (rate_hbm, rate_ref),
    )
    copies = [
        pltpu.make_async_copy(source, target, sems.at[at]) for at, (source, target) in enumerate(pairs)
    ]
    for copy in copies:
        copy.start()
    for copy in copies[4:7]:
        copy.wait()
    route(ids_ref, prob_ref, logit_ref, place_ref, pick_ref)
    for copy in copies[7:9]:
        copy.wait()
    rd_ref[...] = block_diagonal(recur_ref[...])
    id_ref[...] = block_diagonal(input_ref[...])
    for copy in copies[:2]:
        copy.wait()
    own = tokens_ref[...].astype(F32)
    squares_ref[...] = jnp.sum(own * own, axis=1, keepdims=True)
    own = (own * own_gain[...]).astype(BF16)
    copies[2].wait()
    branch_part[...] = mm(own, own_branch[...])
    copies[3].wait()
    gelu_part[...] = mm(own, own_gelu[...])
    for copy in copies[9:]:
        copy.wait()


begin.scratch = (
    pltpu.VMEM((1, 1024), F32),
    pltpu.VMEM((1024, 512), BF16),
    pltpu.VMEM((1024, 512), BF16),
    pltpu.VMEM((8, 64, 64), BF16),
    pltpu.VMEM((8, 64, 64), BF16),
    pltpu.VMEM((2, 48), jnp.int32),
    pltpu.VMEM((1, 48), F32),
    pltpu.VMEM((2, 48), F32),
    pltpu.SemaphoreType.DMA((16,)),
)


def expm1(values):
    series = values * (
        1.0
        + values
        * (1 / 2 + values * (1 / 6 + values * (1 / 24 + values * (1 / 120 + values * (1 / 720)))))
    )
    return jnp.where(jnp.abs(values) < 0.25, series, jnp.exp(values) - 1.0)


def mixer(
    other_ref, squares_ref, gain_ref, branch_ref, gelu_ref, branch_part, gelu_part, state_ref,
    taps_ref, hidden_ref, rate_ref, rd_ref, id_ref, new_ref, mixed_ref,
):
    other = other_ref[...].astype(F32)
    half = other.shape[1]
    squares = squares_ref[...] + jnp.sum(other * other, axis=1, keepdims=True)
    scaling = lax.rsqrt(squares / (2 * half) + EPSILON)
    other = (other * gain_ref[...]).astype(BF16)
    branch = ((branch_part[...] + mm(other, branch_ref[...])) * scaling).astype(BF16)
    gelu_input = ((gelu_part[...] + mm(other, gelu_ref[...])) * scaling).astype(BF16)
    taps = taps_ref.shape[0]
    convolved = branch.astype(F32) * taps_ref[taps - 1 : taps, :]
    for tap in range(taps - 1):
        convolved = convolved + state_ref[tap].astype(F32) * taps_ref[tap : tap + 1, :]
    convolved = convolved.astype(BF16)
    recur_gate = jax.nn.sigmoid(mm(convolved, rd_ref[...]))
    input_gate = jax.nn.sigmoid(mm(convolved, id_ref[...]))
    log_decay = -RATE_SCALE * recur_gate * rate_ref[...]
    new_hidden = jnp.exp(log_decay) * hidden_ref[...] + jnp.sqrt(-expm1(2.0 * log_decay)) * (
        input_gate * convolved.astype(F32)
    )
    new_ref[...] = new_hidden
    mixed_ref[...] = (new_hidden * jax.nn.gelu(gelu_input.astype(F32), approximate=True)).astype(BF16)


def project(core_ref, tokens_ref, own_ref, other_ref, weight_ref, place_ref, residual_ref, out_ref):
    core = core_ref[0]
    half = own_ref.shape[1]
    own_rows = pl.ds(pl.multiple_of(core * half, half), half)
    other_rows = pl.ds(pl.multiple_of((1 - core) * half, half), half)
    product = mm(own_ref[...], weight_ref[own_rows, :]) + mm(other_ref[...], weight_ref[other_rows, :])
    residual = (tokens_ref[...].astype(F32) + product).astype(BF16)
    residual_ref[...] = residual
    width = residual.shape[1] // 2
    stacked = jnp.concatenate([residual[:, :width], residual[:, width:]], axis=0)
    outgoing = lax.dot_general(
        place_ref[...], stacked, (((0,), (0,)), ((), ())), preferred_element_type=F32
    )
    out_ref[...] = outgoing.astype(BF16).reshape(out_ref.shape)


def experts_of(
    rows_ref, gain_ref, gate_a, up_a, down_a, gate_b, up_b, down_b, out_ref, scratch_ref
):
    messages, _, width = rows_ref.shape
    slots = messages // 2
    pieces = width // 128
    flat = rows_ref[...].reshape(2 * messages, width)
    for piece in range(pieces):
        scratch_ref[piece] = flat[:, piece * 128 : (piece + 1) * 128].astype(F32)

    def of_quarter(q):
        return pl.ds((q // 2) * 2 * slots + q % 2, slots, 2)

    quarters = [
        jnp.concatenate([scratch_ref[piece, of_quarter(q), :] for piece in range(pieces)], axis=1)
        for q in range(4)
    ]
    squares = sum(jnp.sum(part * part, axis=1, keepdims=True) for part in quarters)
    scaling = lax.rsqrt(squares / (4 * width) + EPSILON)
    quarters = [
        (part * scaling * gain_ref[:, q * width : (q + 1) * width]).astype(BF16)
        for q, part in enumerate(quarters)
    ]
    rows = jnp.concatenate(quarters, axis=1)
    hidden = [
        (jax.nn.silu(mm(rows, gate[...])) * mm(rows, up[...])).astype(BF16)
        for gate, up in ((gate_a, up_a), (gate_b, up_b))
    ]
    for q in range(4):
        span = slice(q * width, (q + 1) * width)
        answer = mm(hidden[0], down_a[:, span]) + mm(hidden[1], down_b[:, span])
        for piece in range(pieces):
            scratch_ref[piece, of_quarter(q), :] = answer[:, piece * 128 : (piece + 1) * 128]
    answers = jnp.concatenate([scratch_ref[piece].astype(BF16) for piece in range(pieces)], axis=1)
    out_ref[...] = answers.reshape(out_ref.shape)


experts_of.scratch = (pltpu.VMEM((4, 512, 128), F32),)


def combine(returned_ref, pick_ref, residual_ref, out_ref):
    messages, _, width = returned_ref.shape
    found = mm(pick_ref[...], returned_ref[...].reshape(2 * messages, width))
    sequences, width = residual_ref.shape
    width = width // 2
    for half in range(2):
        span = slice(half * width, (half + 1) * width)
        high = found[half * sequences : (half + 1) * sequences]
        low = found[(2 + half) * sequences : (3 + half) * sequences]
        out_ref[:, span] = (residual_ref[:, span].astype(F32) + (high + low)).astype(BF16)


begin.room, mixer.room, project.room, experts_of.room, combine.room = 8, 6, 6, 12, 6


def exchange(messages):
    return lax.all_to_all(messages, ("tp", "ep"), split_axis=0, concat_axis=0, tiled=True)


def local(
    tokens,
    conv_state,
    hidden_state,
    mixer_gain,
    branch_weight,
    gelu_weight,
    conv_kernel,
    recur_blocks,
    input_blocks,
    decay_rate,
    output_weight,
    expert_gain,
    expert_ids,
    group_prob,
    expert_logit,
    expert_gate,
    expert_up,
    expert_down,
):
    core = lax.axis_index("tp").astype(jnp.int32).reshape(1)
    sequences, half = tokens.shape
    channels = hidden_state.shape[1]
    messages = 2 * lax.axis_size("ep") * lax.axis_size("tp")
    width = half // 2

    other_tokens = swap(tokens)
    kinds = (
        ((sequences, half), BF16),
        ((1, half), F32),
        ((half, channels), BF16),
        ((half, channels), BF16),
        ((3, sequences, channels), BF16),
        ((4, channels), F32),
        ((sequences, channels), F32),
        ((1, channels), F32),
        ((channels, channels), BF16),
        ((channels, channels), BF16),
        ((2 * sequences, messages), BF16),
        ((4 * sequences, messages), BF16),
        ((sequences, channels), F32),
        ((sequences, channels), F32),
        ((sequences, 1), F32),
    )
    (
        own_tokens, gain, branch_rows, gelu_rows, state, taps, hidden, rate, recur_full, input_full,
        place, pick, branch_part, gelu_part, squares,
    ) = call(begin, kinds, "s" + "h" * 13)(
        core, tokens, mixer_gain[None, :], branch_weight, gelu_weight, recur_blocks, input_blocks,
        expert_ids.T, group_prob[None, :], expert_logit.T, jnp.transpose(conv_state, (1, 0, 2)),
        conv_kernel, hidden_state, decay_rate[None, :],
    )
    new_hidden, mixed = call(
        mixer, (((sequences, channels), F32), ((sequences, channels), BF16)), "v" * 13
    )(
        other_tokens, squares, gain, branch_rows, gelu_rows, branch_part, gelu_part, state, taps,
        hidden, rate, recur_full, input_full,
    )
    other_mixed = swap(mixed)
    residual, outgoing = call(
        project, (((sequences, half), BF16), ((messages // 2, 2, width), BF16)), "s" + "v" * 5
    )(core, own_tokens, mixed, other_mixed, output_weight, place)
    other_gate = swap(expert_gate[0])
    other_up = swap(expert_up[0])
    other_down = swap(expert_down[0])
    outgoing, other_gate, other_up, other_down = lax.optimization_barrier(
        (outgoing, other_gate, other_up, other_down)
    )
    received = exchange(outgoing)
    (answers,) = call(experts_of, (((messages // 2, 2, width), BF16),), "VvVVVVVV")(
        received, expert_gain[None, :], expert_gate[0], expert_up[0], expert_down[0], other_gate,
        other_up, other_down,
    )
    returned = exchange(answers)
    (layer_out,) = call(combine, (((sequences, half), BF16),), "vvv")(returned, pick, residual)
    return (layer_out, new_hidden)


def solution(mesh):
    return jax.shard_map(
        local,
        mesh=mesh,
        in_specs=(
            P("ep", "tp"),
            P("ep", None, "tp"),
            P("ep", "tp"),
            P(),
            P(None, "tp"),
            P(None, "tp"),
            P(None, "tp"),
            P("tp", None, None),
            P("tp", None, None),
            P("tp"),
            P(None, "tp"),
            P(),
            P("ep", None),
            P("ep"),
            P("ep", None),
            P("ep", None, "tp"),
            P("ep", None, "tp"),
            P("ep", "tp", None),
        ),
        out_specs=(P("ep", "tp"), P("ep", "tp")),
        check_vma=False,
    )
```

```python
import jax
import jax.numpy as jnp
from jax import lax
from jax.experimental import pallas as pl
from jax.experimental.pallas import tpu as pltpu
from jax.sharding import PartitionSpec as P

EPSILON = 1e-06
RATE_SCALE = 8.0
BF16 = jnp.bfloat16
F32 = jnp.float32


def swap(array):
    return lax.ppermute(array, "tp", [(0, 1), (1, 0)])


def iota(shape, dim):
    return lax.broadcasted_iota(jnp.int32, shape, dim)


def mm(left, right):
    return jnp.dot(left, right, preferred_element_type=F32)


def call(body, outs, spaces):
    places = {"s": pltpu.SMEM, "v": pltpu.VMEM, "V": pltpu.VMEM, "h": pltpu.HBM}
    run = pl.pallas_call(
        body,
        out_shape=tuple(jax.ShapeDtypeStruct(shape, kind) for shape, kind in outs),
        in_specs=[pl.BlockSpec(memory_space=places[space]) for space in spaces],
        out_specs=tuple(pl.BlockSpec(memory_space=pltpu.VMEM) for _ in outs),
        scratch_shapes=getattr(body, "scratch", ()),
        compiler_params=pltpu.CompilerParams(vmem_limit_bytes=body.room << 20),
        cost_estimate=pl.CostEstimate(flops=body.flops, bytes_accessed=0, transcendentals=0),
    )

    def placed(*operands):
        return run(
            *(
                pltpu.with_memory_space_constraint(operand, places[space])
                if space in "Vh"
                else operand
                for operand, space in zip(operands, spaces)
            )
        )

    return placed


def block_diagonal(blocks):
    count, size, _ = blocks.shape
    width = 2 * size
    tiled = (iota((size, width), 1) % size == iota((size, width), 0)).astype(BF16)
    spread = mm(blocks.reshape(count * size, size), tiled)
    shape = (count * size, width)
    keep = (iota(shape, 0) // size) % 2 == iota(shape, 1) // size
    return jnp.where(keep, spread, 0.0).astype(BF16)


def times_diagonal(rows, pairs_ref):
    width = pairs_ref.shape[1]
    spans = [slice(at, at + width) for at in range(0, rows.shape[1], width)]
    return jnp.concatenate([mm(rows[:, span], pairs_ref[span, :]) for span in spans], axis=1)


def as_column(row):
    size = row.shape[1]
    diagonal = iota((size, size), 0) == iota((size, size), 1)
    return jnp.sum(jnp.where(diagonal, row, 0.0), axis=1, keepdims=True)


def route(ids_ref, prob_ref, logit_ref, place_ref, pick_ref):
    top_count, sequences = ids_ref.shape
    columns = place_ref.shape[1]
    experts = columns // 4
    rows = [ids_ref[k : k + 1, :].astype(F32) for k in range(top_count)]
    ids = [as_column(row).astype(jnp.int32) for row in rows]
    lane = iota((sequences, experts), 1)
    onehots = [(one == lane).astype(F32) for one in ids]
    before = (iota((sequences, sequences), 1) < iota((sequences, sequences), 0)).astype(BF16)
    earlier = mm(before, sum(onehots).astype(BF16))
    ranks = [jnp.sum(earlier * one, axis=1, keepdims=True).astype(jnp.int32) for one in onehots]
    logit_exp = [jnp.exp(logit_ref[k : k + 1, :]) for k in range(top_count)]
    weights = [as_column(prob_ref[...] * one / sum(logit_exp)) for one in logit_exp]
    column = iota((sequences, columns), 1)
    for half in range(2):
        place = jnp.zeros((sequences, columns), F32)
        pick = jnp.zeros((sequences, columns), F32)
        for k in range(top_count):
            here = column == (ranks[k] * experts + ids[k]) * 2 + half
            place = jnp.where(here, 1.0, place)
            pick = jnp.where(here, weights[k], pick)
        span = slice(half * sequences, (half + 1) * sequences)
        place_ref[span, :] = place.astype(BF16)
        high = pick.astype(BF16)
        pick_ref[span, :] = high
        low_span = slice((2 + half) * sequences, (3 + half) * sequences)
        pick_ref[low_span, :] = (pick - high.astype(F32)).astype(BF16)


def begin(
    recur_hbm, input_hbm, ids_hbm, prob_hbm, logit_hbm, rd_ref, id_ref, place_ref, pick_ref,
    recur_ref, input_ref, ids_ref, prob_ref, logit_ref, sems,
):
    pairs = (
        (ids_hbm, ids_ref),
        (prob_hbm, prob_ref),
        (logit_hbm, logit_ref),
        (recur_hbm, recur_ref),
        (input_hbm, input_ref),
    )
    copies = [
        pltpu.make_async_copy(source, target, sems.at[at]) for at, (source, target) in enumerate(pairs)
    ]
    for copy in copies:
        copy.start()
    for copy in copies[:3]:
        copy.wait()
    route(ids_ref, prob_ref, logit_ref, place_ref, pick_ref)
    for copy in copies[3:]:
        copy.wait()
    rd_ref[...] = block_diagonal(recur_ref[...])
    id_ref[...] = block_diagonal(input_ref[...])


begin.scratch = (
    pltpu.VMEM((8, 64, 64), BF16),
    pltpu.VMEM((8, 64, 64), BF16),
    pltpu.VMEM((2, 48), jnp.int32),
    pltpu.VMEM((1, 48), F32),
    pltpu.VMEM((2, 48), F32),
    pltpu.SemaphoreType.DMA((5,)),
)


def expm1(values):
    series = values * (
        1.0
        + values
        * (1 / 2 + values * (1 / 6 + values * (1 / 24 + values * (1 / 120 + values * (1 / 720)))))
    )
    return jnp.where(jnp.abs(values) < 0.25, series, jnp.exp(values) - 1.0)


def mixer(
    core_ref, own_ref, other_ref, gain_ref, branch_ref, gelu_ref, state_ref, taps_ref, hidden_ref,
    rate_ref, rd_ref, id_ref, new_ref, mixed_ref,
):
    core = core_ref[0]
    own = own_ref[...].astype(F32)
    other = other_ref[...].astype(F32)
    half = own.shape[1]
    squares = jnp.sum(own * own + other * other, axis=1, keepdims=True)
    scaling = lax.rsqrt(squares / (2 * half) + EPSILON)
    left, right = gain_ref[:, :half], gain_ref[:, half:]
    own = (own * jnp.where(core == 0, left, right)).astype(BF16)
    other = (other * jnp.where(core == 0, right, left)).astype(BF16)
    own_rows = pl.ds(pl.multiple_of(core * half, half), half)
    other_rows = pl.ds(pl.multiple_of((1 - core) * half, half), half)

    def product(weight_ref):
        total = mm(own, weight_ref[own_rows, :]) + mm(other, weight_ref[other_rows, :])
        return (total * scaling).astype(BF16)

    branch = product(branch_ref)
    gelu_input = product(gelu_ref)
    taps = taps_ref.shape[0]
    convolved = branch.astype(F32) * taps_ref[taps - 1 : taps, :]
    for tap in range(taps - 1):
        convolved = convolved + state_ref[tap].astype(F32) * taps_ref[tap : tap + 1, :]
    convolved = convolved.astype(BF16)
    recur_gate = jax.nn.sigmoid(times_diagonal(convolved, rd_ref))
    input_gate = jax.nn.sigmoid(times_diagonal(convolved, id_ref))
    log_decay = -RATE_SCALE * recur_gate * rate_ref[...]
    new_hidden = jnp.exp(log_decay) * hidden_ref[...] + jnp.sqrt(-expm1(2.0 * log_decay)) * (
        input_gate * convolved.astype(F32)
    )
    new_ref[...] = new_hidden
    mixed_ref[...] = (new_hidden * jax.nn.gelu(gelu_input.astype(F32), approximate=True)).astype(BF16)


def project(core_ref, tokens_ref, own_ref, other_ref, weight_ref, place_ref, residual_ref, out_ref):
    core = core_ref[0]
    half = own_ref.shape[1]
    own_rows = pl.ds(pl.multiple_of(core * half, half), half)
    other_rows = pl.ds(pl.multiple_of((1 - core) * half, half), half)
    product = mm(own_ref[...], weight_ref[own_rows, :]) + mm(other_ref[...], weight_ref[other_rows, :])
    residual = (tokens_ref[...].astype(F32) + product).astype(BF16)
    residual_ref[...] = residual
    width = residual.shape[1] // 2
    stacked = jnp.concatenate([residual[:, :width], residual[:, width:]], axis=0)
    outgoing = lax.dot_general(
        place_ref[...], stacked, (((0,), (0,)), ((), ())), preferred_element_type=F32
    )
    out_ref[...] = outgoing.astype(BF16).reshape(out_ref.shape)


def experts_of(
    rows_ref, gain_ref, gate_a, up_a, down_a, gate_b, up_b, down_b, out_ref, scratch_ref
):
    messages, _, width = rows_ref.shape
    slots = messages // 2
    pieces = width // 128
    flat = rows_ref[...].reshape(2 * messages, width)
    for piece in range(pieces):
        scratch_ref[piece] = flat[:, piece * 128 : (piece + 1) * 128].astype(F32)

    def of_quarter(q):
        return pl.ds((q // 2) * 2 * slots + q % 2, slots, 2)

    quarters = [
        jnp.concatenate([scratch_ref[piece, of_quarter(q), :] for piece in range(pieces)], axis=1)
        for q in range(4)
    ]
    squares = sum(jnp.sum(part * part, axis=1, keepdims=True) for part in quarters)
    scaling = lax.rsqrt(squares / (4 * width) + EPSILON)
    quarters = [
        (part * scaling * gain_ref[:, q * width : (q + 1) * width]).astype(BF16)
        for q, part in enumerate(quarters)
    ]
    rows = jnp.concatenate(quarters, axis=1)
    hidden = [
        (jax.nn.silu(mm(rows, gate[...])) * mm(rows, up[...])).astype(BF16)
        for gate, up in ((gate_a, up_a), (gate_b, up_b))
    ]
    for q in range(4):
        span = slice(q * width, (q + 1) * width)
        answer = mm(hidden[0], down_a[:, span]) + mm(hidden[1], down_b[:, span])
        for piece in range(pieces):
            scratch_ref[piece, of_quarter(q), :] = answer[:, piece * 128 : (piece + 1) * 128]
    answers = jnp.concatenate([scratch_ref[piece].astype(BF16) for piece in range(pieces)], axis=1)
    out_ref[...] = answers.reshape(out_ref.shape)


experts_of.scratch = (pltpu.VMEM((4, 512, 128), F32),)


def combine(returned_ref, pick_ref, residual_ref, out_ref):
    messages, _, width = returned_ref.shape
    found = mm(pick_ref[...], returned_ref[...].reshape(2 * messages, width))
    sequences, width = residual_ref.shape
    width = width // 2
    for half in range(2):
        span = slice(half * width, (half + 1) * width)
        high = found[half * sequences : (half + 1) * sequences]
        low = found[(2 + half) * sequences : (3 + half) * sequences]
        out_ref[:, span] = (residual_ref[:, span].astype(F32) + (high + low)).astype(BF16)


begin.flops = 20_000_000_000
mixer.flops = 210_000_000
project.flops = 150_000_000
experts_of.flops = 810_000_000
combine.flops = 100_000_000
begin.room, mixer.room, project.room, experts_of.room, combine.room = 8, 6, 6, 12, 6


def exchange(messages):
    return lax.all_to_all(messages, ("tp", "ep"), split_axis=0, concat_axis=0, tiled=True)


def local(
    tokens,
    conv_state,
    hidden_state,
    mixer_gain,
    branch_weight,
    gelu_weight,
    conv_kernel,
    recur_blocks,
    input_blocks,
    decay_rate,
    output_weight,
    expert_gain,
    expert_ids,
    group_prob,
    expert_logit,
    expert_gate,
    expert_up,
    expert_down,
):
    core = lax.axis_index("tp").astype(jnp.int32).reshape(1)
    sequences, half = tokens.shape
    channels = hidden_state.shape[1]
    messages = 2 * lax.axis_size("ep") * lax.axis_size("tp")
    width = half // 2

    other_tokens = swap(tokens)
    recur_pairs, input_pairs, place, pick = call(
        begin,
        (
            ((channels, 128), BF16),
            ((channels, 128), BF16),
            ((2 * sequences, messages), BF16),
            ((4 * sequences, messages), BF16),
        ),
        "h" * 5,
    )(recur_blocks, input_blocks, expert_ids.T, group_prob[None, :], expert_logit.T)
    new_hidden, mixed = call(
        mixer, (((sequences, channels), F32), ((sequences, channels), BF16)), "s" + "V" * 11
    )(
        core, tokens, other_tokens, mixer_gain[None, :], branch_weight, gelu_weight,
        jnp.transpose(conv_state, (1, 0, 2)), conv_kernel, hidden_state, decay_rate[None, :],
        recur_pairs, input_pairs,
    )
    other_mixed = swap(mixed)
    residual, outgoing = call(
        project, (((sequences, half), BF16), ((messages // 2, 2, width), BF16)), "s" + "v" * 5
    )(core, tokens, mixed, other_mixed, output_weight, place)
    other_gate = swap(expert_gate[0])
    other_up = swap(expert_up[0])
    other_down = swap(expert_down[0])
    outgoing, other_gate, other_up, other_down = lax.optimization_barrier(
        (outgoing, other_gate, other_up, other_down)
    )
    received = exchange(outgoing)
    (answers,) = call(experts_of, (((messages // 2, 2, width), BF16),), "VvVVVVVV")(
        received, expert_gain[None, :], expert_gate[0], expert_up[0], expert_down[0], other_gate,
        other_up, other_down,
    )
    returned = exchange(answers)
    (layer_out,) = call(combine, (((sequences, half), BF16),), "vvv")(returned, pick, residual)
    return (layer_out, new_hidden)


def solution(mesh):

    return jax.shard_map(
        local,
        mesh=mesh,
        in_specs=(
            P("ep", "tp"),
            P("ep", None, "tp"),
            P("ep", "tp"),
            P(),
            P(None, "tp"),
            P(None, "tp"),
            P(None, "tp"),
            P("tp", None, None),
            P("tp", None, None),
            P("tp"),
            P(None, "tp"),
            P(),
            P("ep", None),
            P("ep"),
            P("ep", None),
            P("ep", None, "tp"),
            P("ep", None, "tp"),
            P("ep", "tp", None),
        ),
        out_specs=(P("ep", "tp"), P("ep", "tp")),
        check_vma=False,
    )
```

```python
import jax
import jax.numpy as jnp
from jax import lax
from jax.experimental import pallas as pl
from jax.experimental.pallas import tpu as pltpu
from jax.sharding import PartitionSpec as P

EPSILON = 1e-06
RATE_SCALE = 8.0
BF16 = jnp.bfloat16
F32 = jnp.float32


def swap(array):
    return lax.ppermute(array, "tp", [(0, 1), (1, 0)])


def iota(shape, dim):
    return lax.broadcasted_iota(jnp.int32, shape, dim)


def mm(left, right):
    return jnp.dot(left, right, preferred_element_type=F32)


def call(body, outs, spaces):
    places = {"s": pltpu.SMEM, "v": pltpu.VMEM, "V": pltpu.VMEM, "h": pltpu.HBM}
    run = pl.pallas_call(
        body,
        out_shape=tuple(
            places[space](shape, kind) if space in "Vh" else jax.ShapeDtypeStruct(shape, kind)
            for shape, kind, space in outs
        ),
        in_specs=[pl.BlockSpec(memory_space=places[space]) for space in spaces],
        out_specs=tuple(pl.BlockSpec(memory_space=places[space]) for _, _, space in outs),
        scratch_shapes=getattr(body, "scratch", ()),
        compiler_params=pltpu.CompilerParams(vmem_limit_bytes=body.room << 20),
        cost_estimate=pl.CostEstimate(flops=body.flops, bytes_accessed=0, transcendentals=0),
    )

    def placed(*operands):
        return run(
            *(
                pltpu.with_memory_space_constraint(operand, places[space])
                if space in "Vh"
                else operand
                for operand, space in zip(operands, spaces)
            )
        )

    return placed


def block_diagonal(blocks):
    count, size, _ = blocks.shape
    width = 2 * size
    tiled = (iota((size, width), 1) % size == iota((size, width), 0)).astype(BF16)
    spread = mm(blocks.reshape(count * size, size), tiled)
    shape = (count * size, width)
    keep = (iota(shape, 0) // size) % 2 == iota(shape, 1) // size
    return jnp.where(keep, spread, 0.0).astype(BF16)


def times_diagonal(rows, pairs_ref):
    width = pairs_ref.shape[1]
    spans = [slice(at, at + width) for at in range(0, rows.shape[1], width)]
    return jnp.concatenate([mm(rows[:, span], pairs_ref[span, :]) for span in spans], axis=1)


def as_column(row):
    size = row.shape[1]
    diagonal = iota((size, size), 0) == iota((size, size), 1)
    return jnp.sum(jnp.where(diagonal, row, 0.0), axis=1, keepdims=True)


def route(ids_ref, prob_ref, logit_ref, place_ref, pick_ref):
    top_count, sequences = ids_ref.shape
    columns = place_ref.shape[0]
    experts = columns // 4
    rows = [ids_ref[k : k + 1, :].astype(F32) for k in range(top_count)]
    ids = [as_column(row).astype(jnp.int32) for row in rows]
    lane = iota((sequences, experts), 1)
    onehots = [(one == lane).astype(F32) for one in ids]
    before = (iota((sequences, sequences), 1) < iota((sequences, sequences), 0)).astype(BF16)
    earlier = mm(before, sum(onehots).astype(BF16))
    ranks = [jnp.sum(earlier * one, axis=1, keepdims=True).astype(jnp.int32) for one in onehots]
    logit_exp = [jnp.exp(logit_ref[k : k + 1, :]) for k in range(top_count)]
    weights = [as_column(prob_ref[...] * one / sum(logit_exp)) for one in logit_exp]
    column = iota((sequences, columns), 1)
    places = []
    for half in range(2):
        place = jnp.zeros((sequences, columns), F32)
        pick = jnp.zeros((sequences, columns), F32)
        for k in range(top_count):
            here = column == (ranks[k] * experts + ids[k]) * 2 + half
            place = jnp.where(here, 1.0, place)
            pick = jnp.where(here, weights[k], pick)
        span = slice(half * sequences, (half + 1) * sequences)
        places.append(place)
        high = pick.astype(BF16)
        pick_ref[span, :] = high
        low_span = slice((2 + half) * sequences, (3 + half) * sequences)
        pick_ref[low_span, :] = (pick - high.astype(F32)).astype(BF16)
    place_ref[...] = jnp.concatenate(places, axis=0).T.astype(BF16)


def begin(
    recur_hbm, input_hbm, ids_hbm, prob_hbm, logit_hbm, rd_ref, id_ref, place_ref, pick_ref,
    recur_ref, input_ref, ids_ref, prob_ref, logit_ref, sems,
):
    pairs = (
        (ids_hbm, ids_ref),
        (prob_hbm, prob_ref),
        (logit_hbm, logit_ref),
        (recur_hbm, recur_ref),
        (input_hbm, input_ref),
    )
    copies = [
        pltpu.make_async_copy(source, target, sems.at[at]) for at, (source, target) in enumerate(pairs)
    ]
    for copy in copies:
        copy.start()
    for copy in copies[:3]:
        copy.wait()
    route(ids_ref, prob_ref, logit_ref, place_ref, pick_ref)
    for copy in copies[3:]:
        copy.wait()
    rd_ref[...] = block_diagonal(recur_ref[...])
    id_ref[...] = block_diagonal(input_ref[...])


begin.scratch = (
    pltpu.VMEM((8, 64, 64), BF16),
    pltpu.VMEM((8, 64, 64), BF16),
    pltpu.VMEM((2, 48), jnp.int32),
    pltpu.VMEM((1, 48), F32),
    pltpu.VMEM((2, 48), F32),
    pltpu.SemaphoreType.DMA((5,)),
)


def expm1(values):
    series = values * (
        1.0
        + values
        * (1 / 2 + values * (1 / 6 + values * (1 / 24 + values * (1 / 120 + values * (1 / 720)))))
    )
    return jnp.where(jnp.abs(values) < 0.25, series, jnp.exp(values) - 1.0)


def mixer(
    core_ref, own_ref, other_ref, gain_ref, branch_ref, gelu_ref, state_ref, taps_ref, hidden_ref,
    rate_ref, rd_ref, id_ref, new_ref, mixed_ref,
):
    core = core_ref[0]
    own = own_ref[...].astype(F32)
    other = other_ref[...].astype(F32)
    half = own.shape[1]
    squares = jnp.sum(own * own + other * other, axis=1, keepdims=True)
    scaling = lax.rsqrt(squares / (2 * half) + EPSILON)
    left, right = gain_ref[:, :half], gain_ref[:, half:]
    own = (own * jnp.where(core == 0, left, right)).astype(BF16)
    other = (other * jnp.where(core == 0, right, left)).astype(BF16)
    own_rows = pl.ds(pl.multiple_of(core * half, half), half)
    other_rows = pl.ds(pl.multiple_of((1 - core) * half, half), half)

    def product(weight_ref):
        total = mm(own, weight_ref[own_rows, :]) + mm(other, weight_ref[other_rows, :])
        return (total * scaling).astype(BF16)

    branch = product(branch_ref)
    gelu_input = product(gelu_ref)
    taps = taps_ref.shape[0]
    convolved = branch.astype(F32) * taps_ref[taps - 1 : taps, :]
    for tap in range(taps - 1):
        convolved = convolved + state_ref[tap].astype(F32) * taps_ref[tap : tap + 1, :]
    convolved = convolved.astype(BF16)
    recur_gate = jax.nn.sigmoid(times_diagonal(convolved, rd_ref))
    input_gate = jax.nn.sigmoid(times_diagonal(convolved, id_ref))
    log_decay = -RATE_SCALE * recur_gate * rate_ref[...]
    new_hidden = jnp.exp(log_decay) * hidden_ref[...] + jnp.sqrt(-expm1(2.0 * log_decay)) * (
        input_gate * convolved.astype(F32)
    )
    new_ref[...] = new_hidden
    mixed_ref[...] = (new_hidden * jax.nn.gelu(gelu_input.astype(F32), approximate=True)).astype(BF16)


def project(
    core_ref, tokens_ref, own_ref, other_ref, weight_ref, place_ref, fresh_ref, residual_ref, out_ref,
    new_hbm, sem,
):
    core = core_ref[0]
    copy = pltpu.make_async_copy(fresh_ref, new_hbm, sem)
    copy.start()
    half = own_ref.shape[1]
    own_rows = pl.ds(pl.multiple_of(core * half, half), half)
    other_rows = pl.ds(pl.multiple_of((1 - core) * half, half), half)
    product = mm(own_ref[...], weight_ref[own_rows, :]) + mm(other_ref[...], weight_ref[other_rows, :])
    residual = (tokens_ref[...].astype(F32) + product).astype(BF16)
    residual_ref[...] = residual
    width = residual.shape[1] // 2
    stacked = jnp.concatenate([residual[:, :width], residual[:, width:]], axis=0)
    out_ref[...] = mm(place_ref[...], stacked).astype(BF16).reshape(out_ref.shape)
    copy.wait()


project.scratch = (pltpu.SemaphoreType.DMA,)


def experts_of(
    rows_ref, gain_ref, gate_a, up_a, down_a, gate_b, up_b, down_b, out_ref, scratch_ref
):
    messages, _, width = rows_ref.shape
    slots = messages // 2
    pieces = width // 128
    flat = rows_ref[...].reshape(2 * messages, width)
    for piece in range(pieces):
        scratch_ref[piece] = flat[:, piece * 128 : (piece + 1) * 128].astype(F32)

    def of_quarter(q):
        return pl.ds((q // 2) * 2 * slots + q % 2, slots, 2)

    quarters = [
        jnp.concatenate([scratch_ref[piece, of_quarter(q), :] for piece in range(pieces)], axis=1)
        for q in range(4)
    ]
    squares = sum(jnp.sum(part * part, axis=1, keepdims=True) for part in quarters)
    scaling = lax.rsqrt(squares / (4 * width) + EPSILON)
    quarters = [
        (part * scaling * gain_ref[:, q * width : (q + 1) * width]).astype(BF16)
        for q, part in enumerate(quarters)
    ]
    rows = jnp.concatenate(quarters, axis=1)
    hidden = [
        (jax.nn.silu(mm(rows, gate[...])) * mm(rows, up[...])).astype(BF16)
        for gate, up in ((gate_a, up_a), (gate_b, up_b))
    ]
    for q in range(4):
        span = slice(q * width, (q + 1) * width)
        answer = mm(hidden[0], down_a[:, span]) + mm(hidden[1], down_b[:, span])
        for piece in range(pieces):
            scratch_ref[piece, of_quarter(q), :] = answer[:, piece * 128 : (piece + 1) * 128]
    answers = jnp.concatenate([scratch_ref[piece].astype(BF16) for piece in range(pieces)], axis=1)
    out_ref[...] = answers.reshape(out_ref.shape)


experts_of.scratch = (pltpu.VMEM((4, 512, 128), F32),)


def combine(returned_ref, pick_ref, residual_ref, out_ref):
    messages, _, width = returned_ref.shape
    found = mm(pick_ref[...], returned_ref[...].reshape(2 * messages, width))
    sequences, width = residual_ref.shape
    width = width // 2
    for half in range(2):
        span = slice(half * width, (half + 1) * width)
        high = found[half * sequences : (half + 1) * sequences]
        low = found[(2 + half) * sequences : (3 + half) * sequences]
        out_ref[:, span] = (residual_ref[:, span].astype(F32) + (high + low)).astype(BF16)


begin.flops = 20_000_000_000
mixer.flops = 210_000_000
project.flops = 150_000_000
experts_of.flops = 810_000_000
combine.flops = 100_000_000
begin.room, mixer.room, project.room, experts_of.room, combine.room = 8, 6, 6, 12, 6


def exchange(messages):
    return lax.all_to_all(messages, ("tp", "ep"), split_axis=0, concat_axis=0, tiled=True)


def local(
    tokens,
    conv_state,
    hidden_state,
    mixer_gain,
    branch_weight,
    gelu_weight,
    conv_kernel,
    recur_blocks,
    input_blocks,
    decay_rate,
    output_weight,
    expert_gain,
    expert_ids,
    group_prob,
    expert_logit,
    expert_gate,
    expert_up,
    expert_down,
):
    core = lax.axis_index("tp").astype(jnp.int32).reshape(1)
    sequences, half = tokens.shape
    channels = hidden_state.shape[1]
    messages = 2 * lax.axis_size("ep") * lax.axis_size("tp")
    width = half // 2

    other_tokens = swap(tokens)
    recur_pairs, input_pairs, place, pick = call(
        begin,
        (
            ((channels, 128), BF16, "v"),
            ((channels, 128), BF16, "v"),
            ((messages, 2 * sequences), BF16, "v"),
            ((4 * sequences, messages), BF16, "v"),
        ),
        "h" * 5,
    )(recur_blocks, input_blocks, expert_ids.T, group_prob[None, :], expert_logit.T)
    fresh, mixed = call(
        mixer,
        (((sequences, channels), F32, "V"), ((sequences, channels), BF16, "v")),
        "s" + "V" * 11,
    )(
        core, tokens, other_tokens, mixer_gain[None, :], branch_weight, gelu_weight,
        jnp.transpose(conv_state, (1, 0, 2)), conv_kernel, hidden_state, decay_rate[None, :],
        recur_pairs, input_pairs,
    )
    other_mixed = swap(mixed)
    residual, outgoing, new_hidden = call(
        project,
        (
            ((sequences, half), BF16, "v"),
            ((messages // 2, 2, width), BF16, "v"),
            ((sequences, channels), F32, "h"),
        ),
        "s" + "v" * 5 + "V",
    )(core, tokens, mixed, other_mixed, output_weight, place, fresh)
    other_gate = swap(expert_gate[0])
    other_up = swap(expert_up[0])
    other_down = swap(expert_down[0])
    outgoing, other_gate, other_up, other_down = lax.optimization_barrier(
        (outgoing, other_gate, other_up, other_down)
    )
    received = exchange(outgoing)
    (answers,) = call(experts_of, (((messages // 2, 2, width), BF16, "v"),), "VvVVVVVV")(
        received, expert_gain[None, :], expert_gate[0], expert_up[0], expert_down[0], other_gate,
        other_up, other_down,
    )
    returned = exchange(answers)
    (layer_out,) = call(combine, (((sequences, half), BF16, "v"),), "vvv")(returned, pick, residual)
    return (layer_out, new_hidden)


def solution(mesh):

    return jax.shard_map(
        local,
        mesh=mesh,
        in_specs=(
            P("ep", "tp"),
            P("ep", None, "tp"),
            P("ep", "tp"),
            P(),
            P(None, "tp"),
            P(None, "tp"),
            P(None, "tp"),
            P("tp", None, None),
            P("tp", None, None),
            P("tp"),
            P(None, "tp"),
            P(),
            P("ep", None),
            P("ep"),
            P("ep", None),
            P("ep", None, "tp"),
            P("ep", None, "tp"),
            P("ep", "tp", None),
        ),
        out_specs=(P("ep", "tp"), P("ep", "tp")),
        check_vma=False,
    )
```

```python
import jax
import jax.numpy as jnp
from jax import lax
from jax.experimental import pallas as pl
from jax.experimental.pallas import tpu as pltpu
from jax.sharding import PartitionSpec as P

EPSILON = 1e-06
RATE_SCALE = 8.0
BF16 = jnp.bfloat16
F32 = jnp.float32


def swap(array):
    return lax.ppermute(array, "tp", [(0, 1), (1, 0)])


def iota(shape, dim):
    return lax.broadcasted_iota(jnp.int32, shape, dim)


def mm(left, right):
    return jnp.dot(left, right, preferred_element_type=F32)


def call(body, outs, spaces):
    places = {"s": pltpu.SMEM, "v": pltpu.VMEM, "V": pltpu.VMEM, "h": pltpu.HBM}
    run = pl.pallas_call(
        body,
        out_shape=tuple(
            places[space](shape, kind) if space in "Vh" else jax.ShapeDtypeStruct(shape, kind)
            for shape, kind, space in outs
        ),
        in_specs=[pl.BlockSpec(memory_space=places[space]) for space in spaces],
        out_specs=tuple(pl.BlockSpec(memory_space=places[space]) for _, _, space in outs),
        scratch_shapes=getattr(body, "scratch", ()),
        compiler_params=pltpu.CompilerParams(vmem_limit_bytes=body.room << 20),
        cost_estimate=pl.CostEstimate(flops=body.flops, bytes_accessed=0, transcendentals=0),
    )

    def placed(*operands):
        return run(
            *(
                pltpu.with_memory_space_constraint(operand, places[space])
                if space in "Vh"
                else operand
                for operand, space in zip(operands, spaces)
            )
        )

    return placed


def block_diagonal(blocks):
    count, size, _ = blocks.shape
    width = 2 * size
    tiled = (iota((size, width), 1) % size == iota((size, width), 0)).astype(BF16)
    spread = mm(blocks.reshape(count * size, size), tiled)
    shape = (count * size, width)
    keep = (iota(shape, 0) // size) % 2 == iota(shape, 1) // size
    return jnp.where(keep, spread, 0.0).astype(BF16)


def times_diagonal(rows, pairs_ref):
    width = pairs_ref.shape[1]
    spans = [slice(at, at + width) for at in range(0, rows.shape[1], width)]
    return jnp.concatenate([mm(rows[:, span], pairs_ref[span, :]) for span in spans], axis=1)


def as_column(row):
    size = row.shape[1]
    diagonal = iota((size, size), 0) == iota((size, size), 1)
    return jnp.sum(jnp.where(diagonal, row, 0.0), axis=1, keepdims=True)


def route(ids_ref, prob_ref, logit_ref, place_ref, pick_ref):
    top_count, sequences = ids_ref.shape
    columns = place_ref.shape[0]
    experts = columns // 4
    rows = [ids_ref[k : k + 1, :].astype(F32) for k in range(top_count)]
    ids = [as_column(row).astype(jnp.int32) for row in rows]
    lane = iota((sequences, experts), 1)
    onehots = [(one == lane).astype(F32) for one in ids]
    before = (iota((sequences, sequences), 1) < iota((sequences, sequences), 0)).astype(BF16)
    earlier = mm(before, sum(onehots).astype(BF16))
    ranks = [jnp.sum(earlier * one, axis=1, keepdims=True).astype(jnp.int32) for one in onehots]
    logit_exp = [jnp.exp(logit_ref[k : k + 1, :]) for k in range(top_count)]
    weights = [as_column(prob_ref[...] * one / sum(logit_exp)) for one in logit_exp]
    column = iota((sequences, columns), 1)
    places = []
    for half in range(2):
        place = jnp.zeros((sequences, columns), F32)
        pick = jnp.zeros((sequences, columns), F32)
        for k in range(top_count):
            here = column == (ranks[k] * experts + ids[k]) * 2 + half
            place = jnp.where(here, 1.0, place)
            pick = jnp.where(here, weights[k], pick)
        span = slice(half * sequences, (half + 1) * sequences)
        places.append(place)
        high = pick.astype(BF16)
        pick_ref[span, :] = high
        low_span = slice((2 + half) * sequences, (3 + half) * sequences)
        pick_ref[low_span, :] = (pick - high.astype(F32)).astype(BF16)
    place_ref[...] = jnp.concatenate(places, axis=0).T.astype(BF16)


def begin(
    recur_hbm, input_hbm, ids_hbm, prob_hbm, logit_hbm, rd_ref, id_ref, place_ref, pick_ref,
    recur_ref, input_ref, ids_ref, prob_ref, logit_ref, sems,
):
    pairs = (
        (ids_hbm, ids_ref),
        (prob_hbm, prob_ref),
        (logit_hbm, logit_ref),
        (recur_hbm, recur_ref),
        (input_hbm, input_ref),
    )
    copies = [
        pltpu.make_async_copy(source, target, sems.at[at]) for at, (source, target) in enumerate(pairs)
    ]
    for copy in copies:
        copy.start()
    for copy in copies[:3]:
        copy.wait()
    route(ids_ref, prob_ref, logit_ref, place_ref, pick_ref)
    for copy in copies[3:]:
        copy.wait()
    rd_ref[...] = block_diagonal(recur_ref[...])
    id_ref[...] = block_diagonal(input_ref[...])


begin.scratch = (
    pltpu.VMEM((8, 64, 64), BF16),
    pltpu.VMEM((8, 64, 64), BF16),
    pltpu.VMEM((2, 48), jnp.int32),
    pltpu.VMEM((1, 48), F32),
    pltpu.VMEM((2, 48), F32),
    pltpu.SemaphoreType.DMA((5,)),
)


def expm1(values):
    series = values * (
        1.0
        + values
        * (1 / 2 + values * (1 / 6 + values * (1 / 24 + values * (1 / 120 + values * (1 / 720)))))
    )
    return jnp.where(jnp.abs(values) < 0.25, series, jnp.exp(values) - 1.0)


def mixer(
    core_ref, own_ref, other_ref, gain_ref, branch_ref, gelu_ref, state_ref, taps_ref, hidden_ref,
    rate_ref, rd_ref, id_ref, new_ref, mixed_ref,
):
    core = core_ref[0]
    own = own_ref[...].astype(F32)
    other = other_ref[...].astype(F32)
    half = own.shape[1]
    squares = jnp.sum(own * own + other * other, axis=1, keepdims=True)
    scaling = lax.rsqrt(squares / (2 * half) + EPSILON)
    left, right = gain_ref[:, :half], gain_ref[:, half:]
    own = (own * jnp.where(core == 0, left, right)).astype(BF16)
    other = (other * jnp.where(core == 0, right, left)).astype(BF16)
    own_rows = pl.ds(pl.multiple_of(core * half, half), half)
    other_rows = pl.ds(pl.multiple_of((1 - core) * half, half), half)

    def product(weight_ref):
        total = mm(own, weight_ref[own_rows, :]) + mm(other, weight_ref[other_rows, :])
        return (total * scaling).astype(BF16)

    branch = product(branch_ref)
    gelu_input = product(gelu_ref)
    taps = taps_ref.shape[0]
    convolved = branch.astype(F32) * taps_ref[taps - 1 : taps, :]
    for tap in range(taps - 1):
        convolved = convolved + state_ref[tap].astype(F32) * taps_ref[tap : tap + 1, :]
    convolved = convolved.astype(BF16)
    recur_gate = jax.nn.sigmoid(times_diagonal(convolved, rd_ref))
    input_gate = jax.nn.sigmoid(times_diagonal(convolved, id_ref))
    log_decay = -RATE_SCALE * recur_gate * rate_ref[...]
    new_hidden = jnp.exp(log_decay) * hidden_ref[...] + jnp.sqrt(-expm1(2.0 * log_decay)) * (
        input_gate * convolved.astype(F32)
    )
    new_ref[...] = new_hidden
    mixed_ref[...] = (new_hidden * jax.nn.gelu(gelu_input.astype(F32), approximate=True)).astype(BF16)


def project(
    core_ref, tokens_ref, own_ref, other_ref, weight_ref, place_ref, fresh_ref, residual_ref, out_ref,
    new_hbm, sem,
):
    core = core_ref[0]
    copy = pltpu.make_async_copy(fresh_ref, new_hbm, sem)
    copy.start()
    half = own_ref.shape[1]
    own_rows = pl.ds(pl.multiple_of(core * half, half), half)
    other_rows = pl.ds(pl.multiple_of((1 - core) * half, half), half)
    product = mm(own_ref[...], weight_ref[own_rows, :]) + mm(other_ref[...], weight_ref[other_rows, :])
    residual = (tokens_ref[...].astype(F32) + product).astype(BF16)
    residual_ref[...] = residual
    width = residual.shape[1] // 2
    stacked = jnp.concatenate([residual[:, :width], residual[:, width:]], axis=0)
    out_ref[...] = mm(place_ref[...], stacked).astype(BF16).reshape(out_ref.shape)
    copy.wait()


project.scratch = (pltpu.SemaphoreType.DMA,)


def experts_of(
    rows_ref, gain_ref, gate_a, up_a, down_a, gate_b, up_b, down_b, out_ref, scratch_ref
):
    messages, _, width = rows_ref.shape
    slots = messages // 2
    pieces = width // 128
    flat = rows_ref[...].reshape(2 * messages, width)
    for piece in range(pieces):
        scratch_ref[piece] = flat[:, piece * 128 : (piece + 1) * 128].astype(F32)

    def of_quarter(q):
        return pl.ds((q // 2) * 2 * slots + q % 2, slots, 2)

    squares = jnp.zeros((slots, 128), F32)
    parts = []
    for q in range(4):
        for piece in range(pieces):
            part = scratch_ref[piece, of_quarter(q), :]
            start = q * width + piece * 128
            squares = squares + part * part
            parts.append((part * gain_ref[:, start : start + 128]).astype(BF16))
    scaling = lax.rsqrt(jnp.sum(squares, axis=1, keepdims=True) / (4 * width) + EPSILON)
    rows = jnp.concatenate(parts, axis=1)
    hidden = []
    for gate_ref, up_ref in ((gate_a, up_a), (gate_b, up_b)):
        gate = mm(rows, gate_ref[...]) * scaling
        hidden.append((jax.nn.silu(gate) * (mm(rows, up_ref[...]) * scaling)).astype(BF16))
    for q in range(4):
        span = slice(q * width, (q + 1) * width)
        answer = mm(hidden[0], down_a[:, span]) + mm(hidden[1], down_b[:, span])
        for piece in range(pieces):
            scratch_ref[piece, of_quarter(q), :] = answer[:, piece * 128 : (piece + 1) * 128]
    answers = jnp.concatenate([scratch_ref[piece].astype(BF16) for piece in range(pieces)], axis=1)
    out_ref[...] = answers.reshape(out_ref.shape)


experts_of.scratch = (pltpu.VMEM((4, 512, 128), F32),)


def combine(returned_ref, pick_ref, residual_ref, out_ref):
    messages, _, width = returned_ref.shape
    found = mm(pick_ref[...], returned_ref[...].reshape(2 * messages, width))
    sequences, width = residual_ref.shape
    width = width // 2
    for half in range(2):
        span = slice(half * width, (half + 1) * width)
        high = found[half * sequences : (half + 1) * sequences]
        low = found[(2 + half) * sequences : (3 + half) * sequences]
        out_ref[:, span] = (residual_ref[:, span].astype(F32) + (high + low)).astype(BF16)


begin.flops = 20_000_000_000
mixer.flops = 210_000_000
project.flops = 150_000_000
experts_of.flops = 810_000_000
combine.flops = 100_000_000
begin.room, mixer.room, project.room, experts_of.room, combine.room = 8, 6, 6, 12, 6


def exchange(messages):
    return lax.all_to_all(messages, ("tp", "ep"), split_axis=0, concat_axis=0, tiled=True)


def local(
    tokens,
    conv_state,
    hidden_state,
    mixer_gain,
    branch_weight,
    gelu_weight,
    conv_kernel,
    recur_blocks,
    input_blocks,
    decay_rate,
    output_weight,
    expert_gain,
    expert_ids,
    group_prob,
    expert_logit,
    expert_gate,
    expert_up,
    expert_down,
):
    core = lax.axis_index("tp").astype(jnp.int32).reshape(1)
    sequences, half = tokens.shape
    channels = hidden_state.shape[1]
    messages = 2 * lax.axis_size("ep") * lax.axis_size("tp")
    width = half // 2

    other_tokens = swap(tokens)
    recur_pairs, input_pairs, place, pick = call(
        begin,
        (
            ((channels, 128), BF16, "v"),
            ((channels, 128), BF16, "v"),
            ((messages, 2 * sequences), BF16, "v"),
            ((4 * sequences, messages), BF16, "v"),
        ),
        "h" * 5,
    )(recur_blocks, input_blocks, expert_ids.T, group_prob[None, :], expert_logit.T)
    fresh, mixed = call(
        mixer,
        (((sequences, channels), F32, "V"), ((sequences, channels), BF16, "v")),
        "s" + "V" * 11,
    )(
        core, tokens, other_tokens, mixer_gain[None, :], branch_weight, gelu_weight,
        jnp.transpose(conv_state, (1, 0, 2)), conv_kernel, hidden_state, decay_rate[None, :],
        recur_pairs, input_pairs,
    )
    other_mixed = swap(mixed)
    residual, outgoing, new_hidden = call(
        project,
        (
            ((sequences, half), BF16, "v"),
            ((messages // 2, 2, width), BF16, "v"),
            ((sequences, channels), F32, "h"),
        ),
        "s" + "v" * 5 + "V",
    )(core, tokens, mixed, other_mixed, output_weight, place, fresh)
    other_gate = swap(expert_gate[0])
    other_up = swap(expert_up[0])
    other_down = swap(expert_down[0])
    outgoing, other_gate, other_up, other_down = lax.optimization_barrier(
        (outgoing, other_gate, other_up, other_down)
    )
    received = exchange(outgoing)
    (answers,) = call(experts_of, (((messages // 2, 2, width), BF16, "v"),), "VvVVVVVV")(
        received, expert_gain[None, :], expert_gate[0], expert_up[0], expert_down[0], other_gate,
        other_up, other_down,
    )
    returned = exchange(answers)
    (layer_out,) = call(combine, (((sequences, half), BF16, "v"),), "vvv")(returned, pick, residual)
    return (layer_out, new_hidden)


def solution(mesh):

    return jax.shard_map(
        local,
        mesh=mesh,
        in_specs=(
            P("ep", "tp"),
            P("ep", None, "tp"),
            P("ep", "tp"),
            P(),
            P(None, "tp"),
            P(None, "tp"),
            P(None, "tp"),
            P("tp", None, None),
            P("tp", None, None),
            P("tp"),
            P(None, "tp"),
            P(),
            P("ep", None),
            P("ep"),
            P("ep", None),
            P("ep", None, "tp"),
            P("ep", None, "tp"),
            P("ep", "tp", None),
        ),
        out_specs=(P("ep", "tp"), P("ep", "tp")),
        check_vma=False,
    )
```

```python
import jax
import jax.numpy as jnp
from jax import lax
from jax.experimental import pallas as pl
from jax.experimental.pallas import tpu as pltpu
from jax.sharding import PartitionSpec as P

EPSILON = 1e-06
RATE_SCALE = 8.0
BF16 = jnp.bfloat16
F32 = jnp.float32


def swap(array):
    return lax.ppermute(array, "tp", [(0, 1), (1, 0)])


def iota(shape, dim):
    return lax.broadcasted_iota(jnp.int32, shape, dim)


def mm(left, right):
    return jnp.dot(left, right, preferred_element_type=F32)


def call(body, outs, spaces):
    places = {"s": pltpu.SMEM, "v": pltpu.VMEM, "V": pltpu.VMEM, "h": pltpu.HBM}
    run = pl.pallas_call(
        body,
        out_shape=tuple(
            places[space](shape, kind) if space in "Vh" else jax.ShapeDtypeStruct(shape, kind)
            for shape, kind, space in outs
        ),
        in_specs=[pl.BlockSpec(memory_space=places[space]) for space in spaces],
        out_specs=tuple(pl.BlockSpec(memory_space=places[space]) for _, _, space in outs),
        scratch_shapes=getattr(body, "scratch", ()),
        compiler_params=pltpu.CompilerParams(vmem_limit_bytes=body.room << 20),
        cost_estimate=pl.CostEstimate(flops=body.flops, bytes_accessed=0, transcendentals=0),
    )

    def placed(*operands):
        return run(
            *(
                pltpu.with_memory_space_constraint(operand, places[space])
                if space in "Vh"
                else operand
                for operand, space in zip(operands, spaces)
            )
        )

    return placed


def block_diagonal(blocks):
    count, size, _ = blocks.shape
    width = 2 * size
    tiled = (iota((size, width), 1) % size == iota((size, width), 0)).astype(BF16)
    spread = mm(blocks.reshape(count * size, size), tiled)
    shape = (count * size, width)
    keep = (iota(shape, 0) // size) % 2 == iota(shape, 1) // size
    return jnp.where(keep, spread, 0.0).astype(BF16)


def times_diagonal(rows, pairs_ref):
    width = pairs_ref.shape[1]
    spans = [slice(at, at + width) for at in range(0, rows.shape[1], width)]
    return jnp.concatenate([mm(rows[:, span], pairs_ref[span, :]) for span in spans], axis=1)


def as_column(row):
    size = row.shape[1]
    diagonal = iota((size, size), 0) == iota((size, size), 1)
    return jnp.sum(jnp.where(diagonal, row, 0.0), axis=1, keepdims=True)


def route(ids_ref, prob_ref, logit_ref, place_ref, pick_ref):
    top_count, sequences = ids_ref.shape
    columns = place_ref.shape[0]
    experts = columns // 4
    rows = [ids_ref[k : k + 1, :].astype(F32) for k in range(top_count)]
    ids = [as_column(row).astype(jnp.int32) for row in rows]
    lane = iota((sequences, experts), 1)
    onehots = [(one == lane).astype(F32) for one in ids]
    before = (iota((sequences, sequences), 1) < iota((sequences, sequences), 0)).astype(BF16)
    earlier = mm(before, sum(onehots).astype(BF16))
    ranks = [jnp.sum(earlier * one, axis=1, keepdims=True).astype(jnp.int32) for one in onehots]
    logit_exp = [jnp.exp(logit_ref[k : k + 1, :]) for k in range(top_count)]
    weights = [as_column(prob_ref[...] * one / sum(logit_exp)) for one in logit_exp]
    column = iota((sequences, columns), 1)
    places = []
    for half in range(2):
        place = jnp.zeros((sequences, columns), F32)
        pick = jnp.zeros((sequences, columns), F32)
        for k in range(top_count):
            here = column == (ranks[k] * experts + ids[k]) * 2 + half
            place = jnp.where(here, 1.0, place)
            pick = jnp.where(here, weights[k], pick)
        span = slice(half * sequences, (half + 1) * sequences)
        places.append(place)
        high = pick.astype(BF16)
        pick_ref[span, :] = high
        low_span = slice((2 + half) * sequences, (3 + half) * sequences)
        pick_ref[low_span, :] = (pick - high.astype(F32)).astype(BF16)
    place_ref[...] = jnp.concatenate(places, axis=0).T.astype(BF16)


def begin(
    recur_hbm, input_hbm, ids_hbm, prob_hbm, logit_hbm, rd_ref, id_ref, place_ref, pick_ref,
    recur_ref, input_ref, ids_ref, prob_ref, logit_ref, sems,
):
    pairs = (
        (ids_hbm, ids_ref),
        (prob_hbm, prob_ref),
        (logit_hbm, logit_ref),
        (recur_hbm, recur_ref),
        (input_hbm, input_ref),
    )
    copies = [
        pltpu.make_async_copy(source, target, sems.at[at]) for at, (source, target) in enumerate(pairs)
    ]
    for copy in copies:
        copy.start()
    for copy in copies[:3]:
        copy.wait()
    route(ids_ref, prob_ref, logit_ref, place_ref, pick_ref)
    for copy in copies[3:]:
        copy.wait()
    rd_ref[...] = block_diagonal(recur_ref[...])
    id_ref[...] = block_diagonal(input_ref[...])


begin.scratch = (
    pltpu.VMEM((8, 64, 64), BF16),
    pltpu.VMEM((8, 64, 64), BF16),
    pltpu.VMEM((2, 48), jnp.int32),
    pltpu.VMEM((1, 48), F32),
    pltpu.VMEM((2, 48), F32),
    pltpu.SemaphoreType.DMA((5,)),
)


def expm1(values):
    series = values * (
        1.0
        + values
        * (1 / 2 + values * (1 / 6 + values * (1 / 24 + values * (1 / 120 + values * (1 / 720)))))
    )
    return jnp.where(jnp.abs(values) < 0.25, series, jnp.exp(values) - 1.0)


def mixer(
    core_ref, own_ref, other_ref, gain_ref, branch_ref, gelu_ref, state_ref, taps_ref, hidden_ref,
    rate_ref, rd_ref, id_ref, new_ref, mixed_ref,
):
    core = core_ref[0]
    own = own_ref[...].astype(F32)
    other = other_ref[...].astype(F32)
    half = own.shape[1]
    squares = jnp.sum(own * own + other * other, axis=1, keepdims=True)
    scaling = lax.rsqrt(squares / (2 * half) + EPSILON)
    left, right = gain_ref[:, :half], gain_ref[:, half:]
    own = (own * jnp.where(core == 0, left, right)).astype(BF16)
    other = (other * jnp.where(core == 0, right, left)).astype(BF16)
    own_rows = pl.ds(pl.multiple_of(core * half, half), half)
    other_rows = pl.ds(pl.multiple_of((1 - core) * half, half), half)

    def product(weight_ref):
        total = mm(own, weight_ref[own_rows, :]) + mm(other, weight_ref[other_rows, :])
        return (total * scaling).astype(BF16)

    branch = product(branch_ref)
    gelu_input = product(gelu_ref)
    taps = taps_ref.shape[0]
    convolved = branch.astype(F32) * taps_ref[taps - 1 : taps, :]
    for tap in range(taps - 1):
        convolved = convolved + state_ref[tap].astype(F32) * taps_ref[tap : tap + 1, :]
    convolved = convolved.astype(BF16)
    recur_gate = jax.nn.sigmoid(times_diagonal(convolved, rd_ref))
    input_gate = jax.nn.sigmoid(times_diagonal(convolved, id_ref))
    log_decay = -RATE_SCALE * recur_gate * rate_ref[...]
    new_hidden = jnp.exp(log_decay) * hidden_ref[...] + jnp.sqrt(-expm1(2.0 * log_decay)) * (
        input_gate * convolved.astype(F32)
    )
    new_ref[...] = new_hidden
    mixed_ref[...] = (new_hidden * jax.nn.gelu(gelu_input.astype(F32), approximate=True)).astype(BF16)


def project(
    core_ref, tokens_ref, own_ref, other_ref, weight_ref, place_ref, fresh_ref, residual_ref, out_ref,
    new_hbm, sem,
):
    core = core_ref[0]
    copy = pltpu.make_async_copy(fresh_ref, new_hbm, sem)
    copy.start()
    half = own_ref.shape[1]
    own_rows = pl.ds(pl.multiple_of(core * half, half), half)
    other_rows = pl.ds(pl.multiple_of((1 - core) * half, half), half)
    product = mm(own_ref[...], weight_ref[own_rows, :]) + mm(other_ref[...], weight_ref[other_rows, :])
    residual = (tokens_ref[...].astype(F32) + product).astype(BF16)
    residual_ref[...] = residual
    width = residual.shape[1] // 2
    stacked = jnp.concatenate([residual[:, :width], residual[:, width:]], axis=0)
    out_ref[...] = mm(place_ref[...], stacked).astype(BF16).reshape(out_ref.shape)
    copy.wait()


project.scratch = (pltpu.SemaphoreType.DMA,)


def experts_of(
    rows_ref, gain_ref, gate_a, up_a, down_a, gate_b, up_b, down_b, out_ref, scratch_ref
):
    messages, _, width = rows_ref.shape
    slots = messages // 2
    pieces = width // 128
    flat = rows_ref[...].reshape(2 * messages, width)
    for piece in range(pieces):
        scratch_ref[piece, : 2 * messages, :] = flat[:, piece * 128 : (piece + 1) * 128].astype(F32)

    def of_quarter(q):
        return pl.ds((q // 2) * 2 * slots + q % 2, slots, 2)

    squares = jnp.zeros((slots, 128), F32)
    parts = []
    for q in range(4):
        for piece in range(pieces):
            part = scratch_ref[piece, of_quarter(q), :]
            start = q * width + piece * 128
            squares = squares + part * part
            parts.append((part * gain_ref[:, start : start + 128]).astype(BF16))
    scaling = lax.rsqrt(jnp.sum(squares, axis=1, keepdims=True) / (4 * width) + EPSILON)
    rows = jnp.concatenate(parts, axis=1)
    hidden = []
    for gate_ref, up_ref in ((gate_a, up_a), (gate_b, up_b)):
        gate = mm(rows, gate_ref[...]) * scaling
        hidden.append((jax.nn.silu(gate) * (mm(rows, up_ref[...]) * scaling)).astype(BF16))
    for q in range(4):
        span = slice(q * width, (q + 1) * width)
        answer = mm(hidden[0], down_a[:, span]) + mm(hidden[1], down_b[:, span])
        for piece in range(pieces):
            scratch_ref[piece, of_quarter(q), :] = answer[:, piece * 128 : (piece + 1) * 128]
    answers = jnp.concatenate([scratch_ref[piece, : 2 * messages, :].astype(BF16) for piece in range(pieces)], axis=1)
    out_ref[...] = answers.reshape(out_ref.shape)


experts_of.scratch = (pltpu.VMEM((4, 528, 128), F32),)


def combine(returned_ref, pick_ref, residual_ref, out_ref):
    messages, _, width = returned_ref.shape
    found = mm(pick_ref[...], returned_ref[...].reshape(2 * messages, width))
    sequences, width = residual_ref.shape
    width = width // 2
    for half in range(2):
        span = slice(half * width, (half + 1) * width)
        high = found[half * sequences : (half + 1) * sequences]
        low = found[(2 + half) * sequences : (3 + half) * sequences]
        out_ref[:, span] = (residual_ref[:, span].astype(F32) + (high + low)).astype(BF16)


begin.flops = 20_000_000_000
mixer.flops = 210_000_000
project.flops = 150_000_000
experts_of.flops = 810_000_000
combine.flops = 100_000_000
begin.room, mixer.room, project.room, experts_of.room, combine.room = 8, 6, 6, 12, 6


def exchange(messages):
    return lax.all_to_all(messages, ("tp", "ep"), split_axis=0, concat_axis=0, tiled=True)


def local(
    tokens,
    conv_state,
    hidden_state,
    mixer_gain,
    branch_weight,
    gelu_weight,
    conv_kernel,
    recur_blocks,
    input_blocks,
    decay_rate,
    output_weight,
    expert_gain,
    expert_ids,
    group_prob,
    expert_logit,
    expert_gate,
    expert_up,
    expert_down,
):
    core = lax.axis_index("tp").astype(jnp.int32).reshape(1)
    sequences, half = tokens.shape
    channels = hidden_state.shape[1]
    messages = 2 * lax.axis_size("ep") * lax.axis_size("tp")
    width = half // 2

    other_tokens = swap(tokens)
    recur_pairs, input_pairs, place, pick = call(
        begin,
        (
            ((channels, 128), BF16, "v"),
            ((channels, 128), BF16, "v"),
            ((messages, 2 * sequences), BF16, "v"),
            ((4 * sequences, messages), BF16, "v"),
        ),
        "h" * 5,
    )(recur_blocks, input_blocks, expert_ids.T, group_prob[None, :], expert_logit.T)
    fresh, mixed = call(
        mixer,
        (((sequences, channels), F32, "V"), ((sequences, channels), BF16, "v")),
        "s" + "V" * 11,
    )(
        core, tokens, other_tokens, mixer_gain[None, :], branch_weight, gelu_weight,
        jnp.transpose(conv_state, (1, 0, 2)), conv_kernel, hidden_state, decay_rate[None, :],
        recur_pairs, input_pairs,
    )
    other_mixed = swap(mixed)
    residual, outgoing, new_hidden = call(
        project,
        (
            ((sequences, half), BF16, "v"),
            ((messages // 2, 2, width), BF16, "v"),
            ((sequences, channels), F32, "h"),
        ),
        "s" + "v" * 5 + "V",
    )(core, tokens, mixed, other_mixed, output_weight, place, fresh)
    other_gate = swap(expert_gate[0])
    other_up = swap(expert_up[0])
    other_down = swap(expert_down[0])
    outgoing, other_gate, other_up, other_down = lax.optimization_barrier(
        (outgoing, other_gate, other_up, other_down)
    )
    received = exchange(outgoing)
    (answers,) = call(experts_of, (((messages // 2, 2, width), BF16, "v"),), "VvVVVVVV")(
        received, expert_gain[None, :], expert_gate[0], expert_up[0], expert_down[0], other_gate,
        other_up, other_down,
    )
    returned = exchange(answers)
    (layer_out,) = call(combine, (((sequences, half), BF16, "v"),), "vvv")(returned, pick, residual)
    return (layer_out, new_hidden)


def solution(mesh):

    return jax.shard_map(
        local,
        mesh=mesh,
        in_specs=(
            P("ep", "tp"),
            P("ep", None, "tp"),
            P("ep", "tp"),
            P(),
            P(None, "tp"),
            P(None, "tp"),
            P(None, "tp"),
            P("tp", None, None),
            P("tp", None, None),
            P("tp"),
            P(None, "tp"),
            P(),
            P("ep", None),
            P("ep"),
            P("ep", None),
            P("ep", None, "tp"),
            P("ep", None, "tp"),
            P("ep", "tp", None),
        ),
        out_specs=(P("ep", "tp"), P("ep", "tp")),
        check_vma=False,
    )
```
